32 devices in a mesh: ep: 8 (over z, y), tp: 4 (over x, core).
Axes of the slice: x: 2, y: 2, z: 4, core: 2. Of those that a mesh axis runs over, the one named last changes fastest.
Arguments:
- query_rows: bfloat16 [4096, 2048], P('ep', 'tp'), may hold values from -6 to 6
- key_rows: bfloat16 [4096, 512], P('ep', 'tp'), may hold values from -6 to 6
- value_rows: bfloat16 [4096, 512], P('ep', 'tp'), may hold values from -6 to 6
- query_gain: float32 [64], replicated, may hold values from 0.2 to 4.5
- key_gain: float32 [64], replicated, may hold values from 0.2 to 4.5
- sink_logit: float32 [32], P('tp'), may hold values from 2 to 6
- out_weight: bfloat16 [2048, 2048], P('tp'), may hold values from -0.125 to 0.125
- tokens: bfloat16 [4096, 2048], P('ep'), may hold values from -6 to 6
- norm_gain: float32 [2048], replicated, may hold values from 0.1 to 1.9
- expert_ids: int32 [4096, 2], P('ep'), may hold values from 0 to 31, all different within a row; in each aligned block of 128 rows (0 to 127, 128 to 255, ...) at most 16 rows name the same one
- route_weight: float32 [4096, 2], P('ep'), may hold values from 0.2 to 1
- gate_weight: bfloat16 [32, 2048, 1024], P('ep', None, 'tp'), may hold values from -0.125 to 0.125
- up_weight: bfloat16 [32, 2048, 1024], P('ep', None, 'tp'), may hold values from -0.125 to 0.125
- down_weight: bfloat16 [32, 1024, 2048], P('ep', 'tp'), may hold values from -0.1875 to 0.1875
- shared_gate: bfloat16 [2048, 1024], P(None, 'tp'), may hold values from -0.125 to 0.125
- shared_up: bfloat16 [2048, 1024], P(None, 'tp'), may hold values from -0.125 to 0.125
- shared_down: bfloat16 [1024, 2048], P('tp'), may hold values from -0.1875 to 0.1875
Outputs:
- mixer_out: bfloat16 [4096, 2048], P(('ep', 'tp'))
- expert_out: bfloat16 [4096, 2048], P(('ep', 'tp'))
The draws below stay inside these ranges and needn't reach their ends.
Inputs may be any that keep to these rules, and one draw needn't show every extreme that they name: `expert_ids`: each row names 2 different experts. In each aligned block of 128 rows no expert is named by more than 16 rows, a bound that some block reaches.
All inputs are finite; a program needn't handle non-finite values.
Results may differ from the reference program's by a relative error of at most 0.012.
The reference program's roundings to bfloat16 on the way count: a program that leaves them out, or rounds other values in their place, can miss the bound.
Values may be sent and summed in bfloat16 or wider, within the bound.
A program may use at most 128 MiB of HBM per device.

```python
import math
import jax
import jax.numpy as jnp
import numpy as np
from jax import lax

D = 2048
HEADS = 32
KV_HEADS = 8
HEAD_DIM = 64
FF = 1024
WINDOW = 128
BLOCK = 128
TOP_K = 2
B_ROWS = 128
EXPERTS = 32
CAP = 16
TOKENS_A = 4096
TOKENS_B = 4096
N_TP = 4


def attention_pair(key):
    base = jax.random.fold_in(key, 7001)
    first_key, second_key = jax.random.split(base)
    key_values = jax.random.normal(first_key, (TOKENS_A, KV_HEADS * HEAD_DIM), jnp.float32)
    query_values = jax.random.normal(second_key, (TOKENS_A, HEADS * HEAD_DIM), jnp.float32)
    return (jnp.clip(query_values, -6.0, 6.0), jnp.clip(key_values, -6.0, 6.0))


def gain_draw(key):
    return jnp.clip(1.0 + 0.18 * jax.random.normal(key, (HEAD_DIM,), jnp.float32), 0.2, 1.8)


def draw_query_rows(key, part):
    return attention_pair(key)[0].astype(jnp.bfloat16)


def draw_key_rows(key, part):
    return attention_pair(key)[1].astype(jnp.bfloat16)


def draw_query_gain(key, part):
    return gain_draw(jax.random.fold_in(key, 31))


def draw_key_gain(key, part):
    return gain_draw(jax.random.fold_in(key, 47))


def steps_of(stream_key, dims, cuts, low, high):
    factor_of = 1.0
    for axis_at, shards_of in cuts:
        steps = jax.random.uniform(jax.random.fold_in(jax.random.fold_in(stream_key, 6), axis_at), (shards_of,), jnp.float32, low / len(cuts), high / len(cuts))
        factor_of = factor_of * jnp.repeat(jnp.exp(steps), dims[axis_at] // shards_of).reshape((-1,) + (1,) * (len(dims) - 1 - axis_at))
    return factor_of


def assign_block(rng, own, number, rows, amount, top, limit, skew):
    order = jax.random.permutation(rng, amount)
    heavy_load, usual = load_shares(amount, rows * top, limit, skew, True), load_shares(amount, rows * top, limit, skew, False)
    places = jnp.arange(amount)

    def named(tallies, turn):
        used = int((tallies > 0).sum())
        fixed = max(1, used // 4)
        moved = fixed + (places - fixed + turn * (used - fixed)) % max(1, amount - fixed)
        return jnp.zeros((amount,), jnp.int32).at[order[jnp.where(places < fixed, places, moved)]].set(jnp.asarray(tallies, jnp.int32))

    tallies = jnp.where(number % 4 == 0, named(heavy_load, number // 4), named(usual, number - number // 4 - 1))
    mixed = jax.random.permutation(jax.random.fold_in(own, 3), amount)
    giver, taker = mixed[0:amount // 2 * 2:2], mixed[1:amount // 2 * 2:2]
    room = jnp.minimum(tallies[giver] - 1, limit - tallies[taker]) // 2
    room = jnp.where((giver == order[0]) | (taker == order[0]) | (tallies[taker] == 0), 0, jnp.maximum(room, 0))
    moved = jax.random.randint(jax.random.fold_in(own, 4), (amount // 2,), 0, 1 << 20) % (room + 1)
    tallies = tallies.at[giver].add(-moved).at[taker].add(moved)
    labels = jnp.searchsorted(jnp.cumsum(tallies), jnp.arange(rows * top), side="right").astype(jnp.int32)
    listing = labels.reshape(top, rows).T
    listing = listing[jax.random.permutation(jax.random.fold_in(own, 1), rows)]
    turn = jax.random.randint(jax.random.fold_in(own, 2), (rows, 1), 0, top)
    return jnp.take_along_axis(listing, (jnp.arange(top)[None, :] + turn) % top, axis=1)


def load_shares(count, total, limit, lean, full):
    weights = [(1 << 20) // math.isqrt(grade ** lean) + 1 for grade in range(1, count + 1)]
    largest = limit if full else min(limit, max(-(-total // count), total * weights[0] // sum(weights)))
    least = 1 if total - largest >= count - 1 else 0
    given, surplus = [largest] + [least] * (count - 1), total - largest - least * (count - 1)
    while surplus > 0:
        candidates = [i for i in range(1, count) if given[i] < largest] or [i for i in range(1, count) if given[i] < limit]
        pool, remaining = sum([weights[i] for i in candidates]), surplus
        for i in candidates:
            addition = min(limit - given[i], max(1, remaining * weights[i] // pool), surplus)
            given[i] = given[i] + addition
            surplus = surplus - addition
    return np.array(given)


def scatter_about(own_key, extent, width, bound, pieces=(), kind=jnp.bfloat16):
    result = width * jax.random.normal(own_key, extent, jnp.float32)
    if pieces:
        result = result * steps_of(own_key, extent, pieces, -0.22, 0.18)
    return jnp.clip(result, -bound, bound).astype(kind)


def setup_inputs(seed: int = 0) -> dict:
    key_list = jax.random.split(jax.random.key(seed), 18)
    query_rows = draw_query_rows(jax.random.fold_in(key_list[17], 71), 0)
    key_rows = draw_key_rows(jax.random.fold_in(key_list[17], 71), 0)
    value_rows = scatter_about(key_list[2], (TOKENS_A, KV_HEADS * HEAD_DIM), 1.0, 6.0, ((0, 8), (1, 4)))
    query_gain = draw_query_gain(jax.random.fold_in(key_list[17], 71), 0)
    key_gain = draw_key_gain(jax.random.fold_in(key_list[17], 71), 0)
    sink_logit = jnp.clip(2.0 + 4.0 * jax.random.uniform(key_list[5], (HEADS,), jnp.float32) ** steps_of(key_list[5], (HEADS,), ((0, 4),), -0.2, 0.2), 2.0, 6.0)
    out_weight = scatter_about(key_list[6], (HEADS * HEAD_DIM, D), (HEADS * HEAD_DIM) ** -0.5, 0.125, ((0, 4),))
    tokens = scatter_about(key_list[7], (TOKENS_B, D), 1.0, 6.0, ((0, 8),))
    norm_gain = jnp.clip(1.0 + 0.18 * jax.random.normal(key_list[8], (D,), jnp.float32), 0.1, 1.9)
    expert_ids_keys = jax.random.split(jax.random.fold_in(key_list[9], 1), TOKENS_B // B_ROWS)
    expert_ids_turns = jax.random.permutation(jax.random.fold_in(key_list[9], 3), TOKENS_B // B_ROWS)
    expert_ids = jax.vmap(lambda own, number: assign_block(jax.random.fold_in(key_list[9], 2), own, number, B_ROWS, EXPERTS, TOP_K, CAP, 1))(expert_ids_keys, expert_ids_turns).reshape((TOKENS_B, TOP_K))
    route_weight = jnp.clip(0.2 + 0.8 * jax.random.uniform(key_list[10], (TOKENS_B, TOP_K), jnp.float32) ** steps_of(key_list[10], (TOKENS_B, TOP_K), ((0, 8),), -0.2, 0.2), 0.2, 1.0)
    gate_weight = scatter_about(key_list[11], (EXPERTS, D, FF), D ** -0.5, 0.125, ((0, 8), (2, 4)))
    up_weight = scatter_about(key_list[12], (EXPERTS, D, FF), D ** -0.5, 0.125, ((0, 8), (2, 4)))
    down_weight = scatter_about(key_list[13], (EXPERTS, FF, D), FF ** -0.5, 0.1875, ((0, 8), (1, 4)))
    shared_gate = scatter_about(key_list[14], (D, FF), D ** -0.5, 0.125, ((1, 4),))
    shared_up = scatter_about(key_list[15], (D, FF), D ** -0.5, 0.125, ((1, 4),))
    shared_down = scatter_about(key_list[16], (FF, D), FF ** -0.5, 0.1875, ((0, 4),))
    return {"query_rows": query_rows, "key_rows": key_rows, "value_rows": value_rows, "query_gain": query_gain, "key_gain": key_gain, "sink_logit": sink_logit, "out_weight": out_weight, "tokens": tokens, "norm_gain": norm_gain, "expert_ids": expert_ids, "route_weight": route_weight, "gate_weight": gate_weight, "up_weight": up_weight, "down_weight": down_weight, "shared_gate": shared_gate, "shared_up": shared_up, "shared_down": shared_down}


epsilon = 1e-06
masked_score = -1e+30

def rms_scale(values, gain):
    widened = values.astype(jnp.float32)
    scaled = widened * lax.rsqrt(lax.optimization_barrier(jnp.mean(widened * widened, axis=-1, keepdims=True)) + epsilon)
    return (scaled * gain).astype(jnp.bfloat16)

def rounded_sum(hidden, weight):
    group_width = hidden.shape[-1] // N_TP
    running = jnp.zeros((hidden.shape[0], weight.shape[-1]), jnp.float32)
    for group_index in range(N_TP):
        lower = group_index * group_width
        partial_value = jnp.dot(hidden[:, lower:lower + group_width], weight[lower:lower + group_width], preferred_element_type=jnp.float32)
        running = running + lax.optimization_barrier(partial_value.astype(jnp.bfloat16)).astype(jnp.float32)
    return running.astype(jnp.bfloat16)

def expert_ffn(rows_in, gate_matrix, up_matrix, down_matrix):
    gate_part = jnp.dot(rows_in, gate_matrix, preferred_element_type=jnp.float32)
    up_part = jnp.dot(rows_in, up_matrix, preferred_element_type=jnp.float32)
    hidden = (jax.nn.silu(gate_part) * up_part).astype(jnp.bfloat16)
    return rounded_sum(hidden, down_matrix)

def window_mask(first_block, block_count):
    query_pos = jnp.arange(BLOCK)[:, None]
    key_pos = jnp.arange(2 * BLOCK)[None, :]
    inside = (key_pos <= query_pos + BLOCK) & (key_pos > query_pos + BLOCK - WINDOW)
    not_first = (first_block + jnp.arange(block_count))[:, None, None] > 0
    return inside[None] & (not_first | (key_pos[None] >= BLOCK))

def band_blocks(blocks_in):
    earlier = jnp.concatenate([jnp.zeros_like(blocks_in[:1]), blocks_in[:-1]], axis=0)
    return jnp.concatenate([earlier, blocks_in], axis=1)

def reference(query_rows, key_rows, value_rows, query_gain, key_gain, sink_logit, out_weight, tokens, norm_gain, expert_ids, route_weight, gate_weight, up_weight, down_weight, shared_gate, shared_up, shared_down):
    sequence_rows = query_rows.shape[0]
    blocks = sequence_rows // BLOCK
    group_size = HEADS // KV_HEADS
    query_normed = rms_scale(query_rows.reshape(blocks, BLOCK, KV_HEADS, group_size, HEAD_DIM), query_gain)
    key_normed = rms_scale(key_rows.reshape(blocks, BLOCK, KV_HEADS, HEAD_DIM), key_gain)
    key_band = band_blocks(key_normed)
    value_band = band_blocks(value_rows.reshape(blocks, BLOCK, KV_HEADS, HEAD_DIM))
    window = window_mask(0, blocks)
    score_scale = 1.0 / math.sqrt(HEAD_DIM)

    def one_head(inputs):
        query_head, key_head, value_head, sink_head = inputs
        scores = jnp.einsum('nqgd,nkd->gnqk', query_head.astype(jnp.float32), key_head.astype(jnp.float32)) * score_scale
        scores = jnp.where(window[None], scores, masked_score)
        sink_col = sink_head[:, None, None, None]
        row_max = jnp.maximum(lax.optimization_barrier(jnp.max(scores, axis=-1, keepdims=True)), sink_col)
        exp_scores = jnp.exp(scores - row_max)
        attn_probs = (exp_scores / (lax.optimization_barrier(jnp.sum(exp_scores, axis=-1, keepdims=True)) + jnp.exp(sink_col - row_max))).astype(jnp.bfloat16)
        return jnp.einsum('gnqk,nkd->nqgd', attn_probs.astype(jnp.float32), value_head.astype(jnp.float32)).astype(jnp.bfloat16)
    per_head = lax.map(one_head, (jnp.moveaxis(query_normed, 2, 0), jnp.moveaxis(key_band, 2, 0), jnp.moveaxis(value_band, 2, 0), sink_logit.reshape(KV_HEADS, group_size)))
    heads_out = jnp.moveaxis(per_head, 0, 2).reshape(sequence_rows, HEADS * HEAD_DIM)
    mixer_out = rounded_sum(heads_out, out_weight)
    normed = rms_scale(tokens, norm_gain)
    token_count = tokens.shape[0]
    flat_ids = expert_ids.reshape(-1).astype(jnp.int32)
    assign_count = flat_ids.shape[0]
    span_rows = 128
    sort_order = jnp.argsort(flat_ids, stable=True).astype(jnp.int32)
    sorted_ids = flat_ids[sort_order]
    counts = jnp.zeros((EXPERTS,), jnp.int32).at[flat_ids].add(1)
    starts = (jnp.cumsum(counts) - counts).astype(jnp.int32)
    padded = (counts + span_rows - 1) // span_rows * span_rows
    pad_ends = jnp.cumsum(padded).astype(jnp.int32)
    pad_starts = pad_ends - padded
    target = pad_starts[sorted_ids] + jnp.arange(assign_count, dtype=jnp.int32) - starts[sorted_ids]
    span_count = (assign_count + EXPERTS * (span_rows - 1) + span_rows - 1) // span_rows
    slot_assign = jnp.full((span_count * span_rows,), assign_count, jnp.int32).at[target].set(sort_order)
    span_expert = jnp.minimum(jnp.searchsorted(pad_ends, jnp.arange(span_count, dtype=jnp.int32) * span_rows, side='right'), EXPERTS - 1).astype(jnp.int32)
    padded_rows = jnp.concatenate([normed, jnp.zeros((1, D), jnp.bfloat16)], axis=0)

    def one_span(inputs):
        assigns, expert = inputs
        span_tokens = padded_rows[assigns // TOP_K]
        return expert_ffn(span_tokens, gate_weight[expert], up_weight[expert], down_weight[expert])
    span_out = lax.map(one_span, (slot_assign.reshape(span_count, span_rows), span_expert))
    per_assign = jnp.zeros((assign_count + 1, D), jnp.bfloat16).at[slot_assign].set(span_out.reshape(-1, D))
    routed = per_assign[:assign_count].reshape(token_count, TOP_K, D).astype(jnp.float32)
    shared_out = expert_ffn(normed, shared_gate, shared_up, shared_down)
    expert_out = (shared_out.astype(jnp.float32) + lax.optimization_barrier(jnp.sum(routed * route_weight[:, :, None], axis=1))).astype(jnp.bfloat16)
    return (mixer_out, expert_out)
```

```python
import functools
import jax
import jax.numpy as jnp
from jax import lax
from jax.experimental import pallas as pl
from jax.experimental.pallas import tpu as pltpu
from jax.sharding import PartitionSpec as P

HEADS = 32
KV_HEADS = 8
HEAD_DIM = 64
WINDOW = 128
BLOCK = 128
TOP_K = 2


epsilon = 1e-06
masked_score = -1e30
score_scale = 0.125


def from_behind(block, axis, distance):
    devices = range(lax.axis_size(axis))
    route = [(i - distance, i) for i in devices if i - distance in devices]
    return lax.ppermute(block, axis, route)


def rms_scale(values, gain):
    widened = values.astype(jnp.float32)
    scaled = widened * lax.rsqrt(jnp.mean(widened * widened, axis=-1, keepdims=True) + epsilon)
    return (scaled * gain).astype(jnp.bfloat16)


def window_mask(first_block, block_count):
    query_pos = jnp.arange(BLOCK)[:, None]
    key_pos = jnp.arange(2 * BLOCK)[None, :]
    inside = (key_pos <= query_pos + BLOCK) & (key_pos > query_pos + BLOCK - WINDOW)
    not_first = (first_block + jnp.arange(block_count))[:, None, None] > 0
    return inside[None] & (not_first | (key_pos[None] >= BLOCK))


def band_blocks(rim_block, blocks_in):
    joined = jnp.concatenate([rim_block[None], blocks_in], axis=0)
    return jnp.concatenate([joined[:-1], joined[1:]], axis=1)


def layer_kernel(
    ranks,
    near,
    order,
    program,
    local_experts,
    capacity,
    sink,
    query_hbm,
    key_hbm,
    value_hbm,
    query_gain,
    key_gain,
    out_hbm,
    tokens_hbm,
    norm_gain,
    ids_hbm,
    route_hbm,
    gate_hbm,
    up_hbm,
    down_hbm,
    shared_gate_hbm,
    shared_up_hbm,
    shared_down_hbm,
    mixer_out,
    expert_out,
    rows,
    kept,
    sibling_send,
    sibling_recv,
    peer_recv,
    far_out,
    near_out,
    far_back,
    near_back,
    mixer_part,
    shared_part,
    mixer_recv,
    shared_recv,
    mixer_send,
    mixer_peer,
    merged_send,
    merged_recv,
    total,
    tok,
    query,
    key_all,
    value_all,
    key_band,
    value_band,
    heads,
    ids,
    route,
    spots,
    gate,
    up,
    down,
    out_weight,
    shared_gate,
    shared_up,
    shared_down,
    tok_sem,
    small_sem,
    weight_sem,
    rim_send,
    rim_recv,
    out_send,
    out_recv,
    fan_send,
    fan_recv,
    add_send,
    add_recv,
    back_send,
    back_recv,
    early_send,
    early_recv,
):
    rank = lax.axis_index("ep")
    part = lax.axis_index("tp")
    core = lax.rem(part, 2)
    side = part // 2
    sibling = 2 * side + 1 - core
    peer = 2 * (1 - side) + core
    across = 2 * (1 - side) + 1 - core
    placed = (part, peer, sibling, across)
    f32, bf16, i32 = jnp.float32, jnp.bfloat16, jnp.int32
    mesh_ids = pl.DeviceIdType.MESH
    width = rows.shape[-1]
    quarter = tok.shape[1]
    share = rows.shape[2]
    blocks = query.shape[0] // BLOCK
    pairs = query.shape[1] // 128
    spot_of = {k: s for s, k in enumerate(order)}
    chunk = 512
    chunks = width // chunk

    def partner(k):
        result = 0
        bit = 1
        while bit < ranks:
            own = lax.rem(rank // bit, 2)
            result = result + bit * ((1 - own) if k & bit else own)
            bit *= 2
        return result

    def send(source, target, send_sem, recv_sem, ep_to, tp_to):
        copy = pltpu.make_async_remote_copy(
            src_ref=source,
            dst_ref=target,
            send_sem=send_sem,
            recv_sem=recv_sem,
            device_id=(ep_to, tp_to),
            device_id_type=mesh_ids,
        )
        copy.start()
        sent.append(copy)
        return copy

    sent = []
    barrier = pltpu.get_barrier_semaphore()
    ahead = lax.rem(rank + 1, ranks)
    behind = lax.rem(rank + ranks - 1, ranks)
    for k in range(1, ranks):
        pl.semaphore_signal(barrier, inc=1, device_id=(partner(k), part), device_id_type=mesh_ids)
    for other in (sibling, peer):
        pl.semaphore_signal(barrier, inc=1, device_id=(rank, other), device_id_type=mesh_ids)

    def load(source, target, sem):
        copy = pltpu.make_async_copy(source, target, sem)
        copy.start()
        return copy

    def block_at(j):
        return pl.ds(pl.multiple_of(placed[j] * quarter, quarter), quarter)

    tok_loads = [load(tokens_hbm.at[block_at(j)], tok.at[j], tok_sem.at[j]) for j in range(4)]
    id_loads = [load(ids_hbm.at[block_at(j)], ids.at[j], small_sem.at[j]) for j in range(2)]
    sequence = query.shape[0]
    query_load = load(query_hbm, query, small_sem.at[4])
    key_load = load(key_hbm, key_all.at[pl.ds(BLOCK, sequence)], small_sem.at[5])
    value_load = load(value_hbm, value_all.at[pl.ds(BLOCK, sequence)], small_sem.at[6])
    weight_loads = [
        load(source, held, weight_sem.at[i])
        for i, (source, held) in enumerate(
            (
                (out_hbm, out_weight),
                (shared_gate_hbm, shared_gate),
                (shared_up_hbm, shared_up),
                (shared_down_hbm, shared_down),
                (gate_hbm, gate),
                (up_hbm, up),
                (down_hbm, down),
            )
        )
    ]
    route_loads = [load(route_hbm.at[block_at(j)], route.at[j], small_sem.at[2 + j]) for j in range(2)]

    def norm_tokens(j):
        tok_loads[j].wait()
        wide = tok[j].astype(f32)
        scaled = wide * lax.rsqrt(jnp.mean(wide * wide, axis=-1, keepdims=True) + epsilon)
        tok[j] = (scaled * norm_gain[...]).astype(bf16)

    def lay_out(j):
        id_loads[j].wait()
        lanes = lax.broadcasted_iota(i32, (quarter, 128), 1)
        below = (lanes < lax.broadcasted_iota(i32, (quarter, quarter), 0)).astype(bf16)
        columns = [ids[j][:, i : i + 1] for i in range(TOP_K)]
        hot = [(column == lanes).astype(f32) for column in columns]
        before = jnp.dot(below, sum(hot).astype(bf16), preferred_element_type=f32)
        found = []
        for i, column in enumerate(columns):
            within = jnp.sum(hot[i] * before, axis=1, keepdims=True).astype(i32)
            owner = column // local_experts
            ahead_of = 0
            bit = 1
            while bit < ranks:
                own = lax.rem(rank // bit, 2)
                theirs = lax.rem(owner // bit, 2)
                ahead_of = ahead_of + bit * (theirs + own - 2 * theirs * own)
                bit *= 2
            spot = ahead_of * share + lax.rem(column, local_experts) * capacity + within
            spots[j, :, i : i + 1] = spot
            found.append(
                jnp.transpose(jnp.broadcast_to(spot, (quarter, 128)).astype(f32))[0:1, :].astype(i32)
            )
        return found

    def slot_rows(found, j, k, count):
        used = lax.broadcasted_iota(i32, (count * share, quarter), 0) + k * share
        chosen = sum((used == spot).astype(bf16) for spot in found)
        made = jnp.dot(chosen, tok[j], preferred_element_type=f32)
        return made.astype(bf16).reshape(count, share, width)

    dispatched = {}
    to_sibling = {}
    to_peer = {}
    relayed = {}
    added = {}
    peered = {}
    backs = {}

    norm_tokens(0)
    found_own = lay_out(0)
    first_far = True
    rims = []
    for k in range(near, ranks, 2):
        count = min(2, ranks - k)
        far_out[pl.ds(k - near, count)] = slot_rows(found_own, 0, k, count)
        if first_far:
            pl.semaphore_wait(barrier, ranks + 1)
            first_far = False
        for n in range(k, k + count):
            dispatched[n] = send(
                far_out.at[n - near],
                rows.at[spot_of[n], 0],
                out_send.at[n],
                out_recv.at[n],
                partner(n),
                part,
            )
        if k == near:
            key_load.wait()
            value_load.wait()
            tail_rows = pl.ds(sequence, BLOCK)
            rims = [
                send(
                    held.at[tail_rows],
                    held.at[pl.ds(0, BLOCK)],
                    rim_send.at[i],
                    rim_recv.at[i],
                    ahead,
                    part,
                )
                for i, held in enumerate((key_all, value_all))
            ]
            norm_tokens(1)
            found_peer = lay_out(1)
            for n in range(1, near):
                near_out[n - 1, 0:1] = slot_rows(found_own, 0, n, 1)
                near_out[n - 1, 1:2] = slot_rows(found_peer, 1, n, 1)
                dispatched[n] = send(
                    near_out.at[n - 1],
                    rows.at[spot_of[n], pl.ds(0, 2)],
                    out_send.at[n],
                    out_recv.at[n],
                    partner(n),
                    part,
                )
    rows[spot_of[0], 0:1] = slot_rows(found_own, 0, 0, 1)
    rows[spot_of[0], 1:2] = slot_rows(found_peer, 1, 0, 1)

    low = lax.broadcasted_iota(i32, (BLOCK, 128), 1) < HEAD_DIM

    def head_scale(values, gain):
        squares = values * values
        lower = jnp.sum(jnp.where(low, squares, 0.0), axis=1, keepdims=True)
        upper = jnp.sum(jnp.where(low, 0.0, squares), axis=1, keepdims=True)
        mean = jnp.where(low, lower, upper) * (1.0 / HEAD_DIM)
        return values * lax.rsqrt(mean + epsilon) * gain

    def doubled(gain):
        return jnp.concatenate([gain[...], gain[...]], axis=1)

    def band_block(index, carry):
        at = pl.ds(pl.multiple_of(index * BLOCK, BLOCK), BLOCK)
        keys = head_scale(key_all[at].astype(f32), doubled(key_gain))
        values = value_all[at].astype(f32)
        for wide, band in ((keys, key_band), (values, value_band)):
            turned = pltpu.roll(wide, HEAD_DIM, 1)
            band[0, 0, at] = jnp.where(low, wide, 0.0).astype(bf16)
            band[0, 1, at] = jnp.where(low, 0.0, turned).astype(bf16)
            band[1, 0, at] = jnp.where(low, turned, 0.0).astype(bf16)
            band[1, 1, at] = jnp.where(low, 0.0, wide).astype(bf16)
        return carry

    def attend(n, slot):
        at = pl.ds(pl.multiple_of(n * BLOCK, BLOCK), BLOCK)
        span = pl.ds(pl.multiple_of(n * BLOCK, BLOCK), 2 * BLOCK)
        query_pos = lax.broadcasted_iota(i32, (BLOCK, 2 * BLOCK), 0)
        key_pos = lax.broadcasted_iota(i32, (BLOCK, 2 * BLOCK), 1)
        floor = jnp.where(rank * blocks + n > 0, 0, BLOCK)
        inside = (key_pos <= query_pos + BLOCK) & (key_pos > query_pos + BLOCK - WINDOW)
        inside = inside & (key_pos >= floor)
        for pair in range(pairs):
            kv = pair * 2 // (HEADS // KV_HEADS)
            lanes = slice(pair * 128, pair * 128 + 128)
            normed = head_scale(query[at, lanes].astype(f32), doubled(query_gain)).astype(bf16)
            keys = key_band[kv, :, span].reshape(4 * BLOCK, 128)
            scores = lax.dot_general(
                normed, keys, (((1,), (1,)), ((), ())), preferred_element_type=f32
            )
            probs = []
            for h in range(2):
                logit = sink[2 * pair + h]
                score = scores[:, h * 2 * BLOCK : (h + 1) * 2 * BLOCK] * score_scale
                score = jnp.where(inside, score, masked_score)
                top = jnp.maximum(jnp.max(score, axis=1, keepdims=True), logit)
                raised = jnp.exp(score - top)
                below = jnp.sum(raised, axis=1, keepdims=True) + jnp.exp(logit - top)
                probs.append((raised * (1.0 / below)).astype(bf16))
            values = value_band[kv, :, span].reshape(4 * BLOCK, 128)
            made = jnp.dot(jnp.concatenate(probs, axis=1), values, preferred_element_type=f32)
            heads[slot, :, lanes] = made.astype(bf16)

    def attention():
        query_load.wait()
        lax.fori_loop(1, blocks + 1, band_block, 0)
        for rim in rims:
            rim.wait_recv()
        band_block(0, 0)

        def one(j, carry):
            high = lax.rem(j, 2)
            turn = j // 2
            n = 2 * (side + high - 2 * side * high) + core + turn - 2 * core * turn
            attend(n, j)
            return carry

        lax.fori_loop(0, 4, one, 0)

    def early_pair(i, full, received):
        return send(
            full.at[pl.ds(2, 2)], received, early_send.at[i], early_recv.at[i], rank, sibling
        )

    early = {}

    def mixer():
        weight_loads[0].wait()
        for half in (1, 0):
            held = heads[2 * half : 2 * half + 2].reshape(2 * quarter, heads.shape[-1])

            def one(c, carry):
                at = pl.ds(pl.multiple_of(c * chunk, chunk), chunk)
                made = jnp.dot(held, out_weight[:, at], preferred_element_type=f32)
                mixer_part[2 * half : 2 * half + 2, :, at] = made.astype(bf16).reshape(
                    2, quarter, chunk
                )
                return carry

            lax.fori_loop(0, chunks, one, 0)
            if half:
                early["mixer"] = early_pair(0, mixer_part, mixer_recv)

    def shared():
        for i in (1, 2, 3):
            weight_loads[i].wait()
        for half in (1, 0):
            held = tok[2 * half : 2 * half + 2].reshape(2 * quarter, width)
            gate_part = jnp.dot(held, shared_gate[...], preferred_element_type=f32)
            up_part = jnp.dot(held, shared_up[...], preferred_element_type=f32)
            hidden = (gate_part / (1.0 + jnp.exp(-gate_part)) * up_part).astype(bf16)

            def one(c, carry):
                at = pl.ds(pl.multiple_of(c * chunk, chunk), chunk)
                made = jnp.dot(hidden, shared_down[:, at], preferred_element_type=f32)
                shared_part[2 * half : 2 * half + 2, :, at] = made.astype(bf16).reshape(
                    2, quarter, chunk
                )
                return carry

            lax.fori_loop(0, chunks, one, 0)
            if half:
                early["shared"] = early_pair(1, shared_part, shared_recv)

    def mixer_add():
        early["mixer"].wait_recv()
        mixer_send[...] = (mixer_part[1].astype(f32) + mixer_recv[1].astype(f32)).astype(bf16)
        early["peer"] = send(
            mixer_send, mixer_peer, early_send.at[2], early_recv.at[2], rank, peer
        )

    def mixer_finish():
        early["peer"].wait_recv()
        mixer_out[...] = (
            mixer_part[0].astype(f32) + mixer_recv[0].astype(f32) + mixer_peer[...].astype(f32)
        ).astype(bf16)

    def pass_on(k, sem, which, count):
        s = spot_of[k]
        return send(
            rows.at[s, pl.ds(which, count)],
            rows.at[s, pl.ds(2 + which, count)],
            fan_send.at[sem, k],
            fan_recv.at[sem, k],
            rank,
            sibling,
        )

    def fan(k):
        s = spot_of[k]
        if k:
            dispatched[k].wait_recv()
        if k >= near:
            to_peer[k] = send(
                rows.at[s, 0], rows.at[s, 1], fan_send.at[0, k], fan_recv.at[0, k], rank, peer
            )
            to_sibling[k] = pass_on(k, 1, 0, 1)
        else:
            to_sibling[k] = pass_on(k, 1, 0, 2)

    def relay(k):
        to_peer[k].wait_recv()
        relayed[k] = pass_on(k, 2, 1, 1)

    ready = []

    def experts(*names):
        count = len(names)
        first = spot_of[names[0]]
        for k in names:
            to_sibling[k].wait_recv()
            if k in relayed:
                relayed[k].wait_recv()
        if not ready:
            for i in (4, 5, 6):
                weight_loads[i].wait()
            ready.append(True)

        def one(index, carry):
            at = pl.ds(pl.multiple_of(index * capacity, capacity), capacity)
            block = rows[first : first + count, :, at, :].reshape(count * 4 * capacity, width)
            gate_part = jnp.dot(block, gate[index], preferred_element_type=f32)
            up_part = jnp.dot(block, up[index], preferred_element_type=f32)
            hidden = (gate_part / (1.0 + jnp.exp(-gate_part)) * up_part).astype(bf16)
            made = jnp.dot(hidden, down[index], preferred_element_type=f32)
            made = made.astype(bf16).reshape(count, 4, capacity, width)
            spot = pl.ds(first, count)
            kept[spot, :, at, :] = made[:, 0:2]
            sibling_send[spot, :, at, :] = made[:, 2:4]
            return carry

        lax.fori_loop(0, local_experts, one, 0)
        for k in names:
            s = spot_of[k]
            added[k] = send(
                sibling_send.at[s],
                sibling_recv.at[s],
                add_send.at[0, k],
                add_recv.at[0, k],
                rank,
                sibling,
            )

    def add_pair(k):
        s = spot_of[k]
        added[k].wait_recv()
        if k >= near:
            kept[s, 1] = (kept[s, 1].astype(f32) + sibling_recv[s, 1].astype(f32)).astype(bf16)
            peered[k] = send(
                kept.at[s, 1],
                peer_recv.at[k - near],
                add_send.at[1, k],
                add_recv.at[1, k],
                rank,
                peer,
            )
            return
        both = (kept[s].astype(f32) + sibling_recv[s].astype(f32)).astype(bf16)
        if k == 0:
            near_back[0] = both
            return
        kept[s] = both
        backs[k] = send(
            kept.at[s], near_back.at[k], back_send.at[k], back_recv.at[k], partner(k), part
        )

    def finish(k):
        s = spot_of[k]
        peered[k].wait_recv()
        kept[s, 0] = (
            kept[s, 0].astype(f32)
            + sibling_recv[s, 0].astype(f32)
            + peer_recv[k - near].astype(f32)
        ).astype(bf16)
        backs[k] = send(
            kept.at[s, 0], far_back.at[k - near], back_send.at[k], back_recv.at[k], partner(k), part
        )

    def picked(j, source, first):
        count = source.shape[0]
        slots = lax.broadcasted_iota(i32, (quarter, count), 1) + first
        result = 0
        for i in range(TOP_K):
            hot = (spots[j, :, i : i + 1] == slots).astype(bf16)
            result = result + jnp.dot(hot, source, preferred_element_type=f32) * route[
                j, :, i : i + 1
            ]
        return result

    def near_sum(j):
        if j:
            for k in range(1, near):
                backs[k].wait_recv()
            early["shared"].wait_recv()
            for copy in route_loads:
                copy.wait()

        def one(c, carry):
            at = pl.ds(pl.multiple_of(c * chunk, chunk), chunk)
            source = near_back[:, j, :, at].reshape(near * share, chunk)
            value = (
                shared_part[j, :, at].astype(f32)
                + shared_recv[j, :, at].astype(f32)
                + picked(j, source, 0)
            )
            if j:
                merged_send[:, at] = value.astype(bf16)
            else:
                total[:, at] = value
            return carry

        lax.fori_loop(0, chunks, one, 0)
        if j:
            early["merged"] = send(
                merged_send, merged_recv, early_send.at[3], early_recv.at[3], rank, peer
            )

    def far_sum(first, count, last):
        for k in range(first, first + count):
            backs[k].wait_recv()
        if last:
            early["merged"].wait_recv()

        def one(c, carry):
            at = pl.ds(pl.multiple_of(c * chunk, chunk), chunk)
            source = far_back[first - near : first - near + count, :, at].reshape(
                count * share, chunk
            )
            value = total[:, at] + picked(0, source, first * share)
            if last:
                value = value + merged_recv[:, at].astype(f32)
                expert_out[:, at] = value.astype(bf16)
            else:
                total[:, at] = value
            return carry

        lax.fori_loop(0, chunks, one, 0)

    steps = {
        "norm": norm_tokens,
        "attention": attention,
        "mixer": mixer,
        "shared": shared,
        "mixer_add": mixer_add,
        "mixer_finish": mixer_finish,
        "fan": fan,
        "relay": relay,
        "experts": experts,
        "add": add_pair,
        "finish": finish,
        "near_sum": near_sum,
        "far_sum": far_sum,
    }
    for name, *settings in program:
        steps[name](*settings)
    for copy in sent:
        copy.wait_send()


def step_order(ranks, near):
    half = (ranks - near) // 2
    program = [("fan", 0), ("attention",), ("fan", 4), ("fan", 1), ("norm", 2), ("norm", 3)]
    program += [("mixer",), ("relay", 4), ("shared",), ("mixer_add",), ("fan", 2)]
    program += [("experts", 0, 1), ("fan", 5), ("mixer_finish",), ("add", 0), ("add", 1)]
    program += [("relay", 5), ("experts", 4, 2), ("fan", 3), ("fan", 6)]
    program += [("add", 4), ("add", 2), ("relay", 6), ("experts", 5, 3), ("finish", 4)]
    program += [("fan", 7), ("add", 5), ("add", 3), ("relay", 7), ("finish", 5)]
    program += [("experts", 6, 7), ("add", 6), ("add", 7), ("near_sum", 1), ("near_sum", 0)]
    program += [("finish", 6), ("finish", 7), ("far_sum", 4, half, False)]
    program += [("far_sum", 4 + half, half, True)]
    return program


def layer(arrays, local_experts, capacity, ranks):
    query_rows, out_weight, tokens, gate, up, down, shared_gate, shared_up, shared_down = arrays[1]
    near = 4
    order = (0, 1, 4, 2, 5, 3, 6, 7)
    bf16, f32 = jnp.bfloat16, jnp.float32
    dma = pltpu.SemaphoreType.DMA
    quarter = tokens.shape[0] // 4
    width = tokens.shape[1]
    share = local_experts * capacity
    sequence = query_rows.shape[0]
    far = ranks - near
    vmem = pl.BlockSpec(memory_space=pltpu.VMEM)
    anywhere = pl.BlockSpec(memory_space=pl.ANY)
    smem = pl.BlockSpec(memory_space=pltpu.SMEM)

    def held(*shape):
        return pltpu.VMEM(shape, bf16)

    return pl.pallas_call(
        functools.partial(
            layer_kernel, ranks, near, order, step_order(ranks, near), local_experts, capacity
        ),
        out_shape=(
            jax.ShapeDtypeStruct((quarter, width), bf16),
            jax.ShapeDtypeStruct((quarter, width), bf16),
        ),
        in_specs=[smem]
        + [anywhere] * 3
        + [vmem] * 2
        + [anywhere] * 2
        + [vmem]
        + [anywhere] * 8,
        out_specs=(vmem, vmem),
        scratch_shapes=[
            held(ranks, 4, share, width),
            held(ranks, 2, share, width),
            held(ranks, 2, share, width),
            held(ranks, 2, share, width),
            held(far, share, width),
            held(far, share, width),
            held(near - 1, 2, share, width),
            held(far, share, width),
            held(near, 2, share, width),
            held(4, quarter, width),
            held(4, quarter, width),
            held(2, quarter, width),
            held(2, quarter, width),
            held(quarter, width),
            held(quarter, width),
            held(quarter, width),
            held(quarter, width),
            pltpu.VMEM((quarter, width), f32),
            held(4, quarter, width),
            held(*query_rows.shape),
            held(sequence + BLOCK, 128),
            held(sequence + BLOCK, 128),
            held(2, 2, sequence + BLOCK, 128),
            held(2, 2, sequence + BLOCK, 128),
            held(4, quarter, query_rows.shape[1]),
            pltpu.VMEM((2, quarter, TOP_K), jnp.int32),
            pltpu.VMEM((2, quarter, TOP_K), f32),
            pltpu.VMEM((2, quarter, TOP_K), jnp.int32),
            held(*gate.shape),
            held(*up.shape),
            held(*down.shape),
            held(*out_weight.shape),
            held(*shared_gate.shape),
            held(*shared_up.shape),
            held(*shared_down.shape),
            dma((4,)),
            dma((7,)),
            dma((7,)),
            dma((2,)),
            dma((2,)),
            dma((ranks,)),
            dma((ranks,)),
            dma((3, ranks)),
            dma((3, ranks)),
            dma((2, ranks)),
            dma((2, ranks)),
            dma((ranks,)),
            dma((ranks,)),
            dma((4,)),
            dma((4,)),
        ],
        compiler_params=pltpu.CompilerParams(
            collective_id=0, has_side_effects=True, vmem_limit_bytes=65000 * 1024
        ),
    )(*arrays[0])


def wide_shards(
    query_rows,
    key_rows,
    value_rows,
    query_gain,
    key_gain,
    sink_logit,
    out_weight,
    tokens,
    norm_gain,
    expert_ids,
    route_weight,
    gate_weight,
    up_weight,
    down_weight,
    shared_gate,
    shared_up,
    shared_down,
):
    expert_ranks = lax.axis_size("ep")
    head_ranks = lax.axis_size("tp")
    head_rank = lax.axis_index("tp")
    sequence_rows = query_rows.shape[0]
    blocks = sequence_rows // BLOCK
    pair_heads = key_rows.shape[1] // HEAD_DIM
    group_size = HEADS // KV_HEADS
    query_normed = rms_scale(
        query_rows.reshape(blocks, BLOCK, pair_heads, group_size, HEAD_DIM), query_gain
    )
    key_normed = rms_scale(key_rows.reshape(blocks, BLOCK, pair_heads, HEAD_DIM), key_gain)
    value_blocks = value_rows.reshape(blocks, BLOCK, pair_heads, HEAD_DIM)
    rim_keys, rim_values = from_behind((key_normed[blocks - 1], value_blocks[blocks - 1]), "ep", 1)
    key_band = band_blocks(rim_keys, key_normed)
    value_band = band_blocks(rim_values, value_blocks)
    window = window_mask(lax.axis_index("ep") * blocks, blocks)
    scores = (
        jnp.einsum("nqhgd,nkhd->hgnqk", query_normed, key_band, preferred_element_type=jnp.float32)
        * score_scale
    )
    scores = jnp.where(window[None, None], scores, masked_score)
    sink_col = sink_logit.reshape(pair_heads, group_size, 1, 1, 1)
    row_max = jnp.maximum(jnp.max(scores, axis=-1, keepdims=True), sink_col)
    exp_scores = jnp.exp(scores - row_max)
    attn_probs = (
        exp_scores / (jnp.sum(exp_scores, axis=-1, keepdims=True) + jnp.exp(sink_col - row_max))
    ).astype(jnp.bfloat16)
    heads_out = (
        jnp.einsum("hgnqk,nkhd->nqhgd", attn_probs, value_band, preferred_element_type=jnp.float32)
        .astype(jnp.bfloat16)
        .reshape(sequence_rows, pair_heads * group_size * HEAD_DIM)
    )
    local_experts = gate_weight.shape[0]
    expert_total = local_experts * expert_ranks
    quarter = tokens.shape[0] // head_ranks
    model_width = tokens.shape[1]
    capacity = 2 * quarter * TOP_K // expert_total
    slot_share = local_experts * capacity
    routed_rows = expert_ranks * slot_share
    normed = rms_scale(tokens, norm_gain)
    route_ids = expert_ids.reshape(head_ranks, quarter * TOP_K)
    one_hot = (route_ids[:, :, None] == jnp.arange(expert_total, dtype=jnp.int32)).astype(jnp.int32)
    slot_rank = jnp.sum(one_hot * (jnp.cumsum(one_hot, axis=1) - 1), axis=-1)
    positions = route_ids * capacity + slot_rank
    owners = jnp.arange(quarter * TOP_K, dtype=jnp.int32) // TOP_K
    padded_rows = jnp.concatenate(
        [
            normed.reshape(head_ranks, quarter, model_width),
            jnp.zeros((head_ranks, 1, model_width), jnp.bfloat16),
        ],
        axis=1,
    ).reshape(head_ranks * (quarter + 1), model_width)
    slot_token = (
        jnp.full((head_ranks, routed_rows), quarter, jnp.int32)
        .at[jnp.arange(head_ranks, dtype=jnp.int32)[:, None], positions]
        .set(jnp.broadcast_to(owners[None, :], positions.shape))
    )
    slot_index = slot_token + (jnp.arange(head_ranks, dtype=jnp.int32) * (quarter + 1))[:, None]
    own_index = lax.dynamic_index_in_dim(slot_index, head_rank, 0, keepdims=True)
    outgoing = padded_rows[own_index].reshape(1, expert_ranks, slot_share, model_width)
    arrived = lax.all_to_all(outgoing, "ep", split_axis=1, concat_axis=1, tiled=True)
    piece_rows = lax.all_gather(
        arrived.reshape(1, expert_ranks, local_experts, capacity, model_width),
        "tp",
        axis=0,
        tiled=True,
    )
    gate_part = jnp.einsum(
        "tsecd,edf->tsecf", piece_rows, gate_weight, preferred_element_type=jnp.float32
    )
    up_part = jnp.einsum(
        "tsecd,edf->tsecf", piece_rows, up_weight, preferred_element_type=jnp.float32
    )
    hidden = (jax.nn.silu(gate_part) * up_part).astype(jnp.bfloat16)
    shared_hidden = (
        jax.nn.silu(jnp.dot(normed, shared_gate, preferred_element_type=jnp.float32))
        * jnp.dot(normed, shared_up, preferred_element_type=jnp.float32)
    ).astype(jnp.bfloat16)
    span_rows = routed_rows + quarter
    mixer_out = lax.psum_scatter(
        jnp.dot(heads_out, out_weight, preferred_element_type=jnp.float32).astype(jnp.bfloat16),
        "tp",
        scatter_dimension=0,
        tiled=True,
    )
    part_count = lax.axis_size("tp") * span_rows // span_rows
    routed_part = jnp.einsum(
        "tsecf,efd->tsecd", hidden, down_weight, preferred_element_type=jnp.float32
    ).reshape(part_count, routed_rows, model_width)
    shared_part = jnp.dot(shared_hidden, shared_down, preferred_element_type=jnp.float32).reshape(
        part_count, quarter, model_width
    )
    summed = lax.psum_scatter(
        jnp.concatenate([routed_part, shared_part], axis=1)
        .reshape(part_count * span_rows, model_width)
        .astype(jnp.bfloat16),
        "tp",
        scatter_dimension=0,
        tiled=True,
    )
    returned = lax.all_to_all(
        summed[:routed_rows].reshape(expert_ranks, slot_share, model_width),
        "ep",
        split_axis=0,
        concat_axis=0,
        tiled=True,
    ).reshape(routed_rows, model_width)
    own_positions = lax.dynamic_index_in_dim(positions, head_rank, 0, keepdims=False)
    picked = returned[own_positions].reshape(quarter, TOP_K, model_width).astype(jnp.float32)
    own_weights = lax.dynamic_slice_in_dim(route_weight, head_rank * quarter, quarter, 0)
    expert_out = (
        summed[routed_rows:].astype(jnp.float32) + jnp.sum(picked * own_weights[:, :, None], axis=1)
    ).astype(jnp.bfloat16)
    return (mixer_out, expert_out)


def shards(
    query_rows,
    key_rows,
    value_rows,
    query_gain,
    key_gain,
    sink_logit,
    out_weight,
    tokens,
    norm_gain,
    expert_ids,
    route_weight,
    gate_weight,
    up_weight,
    down_weight,
    shared_gate,
    shared_up,
    shared_down,
):
    expert_ranks = lax.axis_size("ep")
    head_ranks = lax.axis_size("tp")
    local_experts = gate_weight.shape[0]
    expert_total = local_experts * expert_ranks
    quarter = tokens.shape[0] // head_ranks
    capacity = 2 * quarter * TOP_K // expert_total
    fits = (
        head_ranks == 4
        and expert_ranks == 8
        and capacity % 16 == 0
        and quarter == BLOCK
        and query_rows.shape[0] == 4 * BLOCK
        and key_rows.shape[1] == 2 * HEAD_DIM
    )
    if not fits:
        return wide_shards(
            query_rows,
            key_rows,
            value_rows,
            query_gain,
            key_gain,
            sink_logit,
            out_weight,
            tokens,
            norm_gain,
            expert_ids,
            route_weight,
            gate_weight,
            up_weight,
            down_weight,
            shared_gate,
            shared_up,
            shared_down,
        )
    operands = (
        sink_logit,
        query_rows,
        key_rows,
        value_rows,
        query_gain.reshape(1, HEAD_DIM),
        key_gain.reshape(1, HEAD_DIM),
        out_weight,
        tokens,
        norm_gain.reshape(1, tokens.shape[1]),
        expert_ids,
        route_weight,
        gate_weight,
        up_weight,
        down_weight,
        shared_gate,
        shared_up,
        shared_down,
    )
    shaped = (
        query_rows,
        out_weight,
        tokens,
        gate_weight,
        up_weight,
        down_weight,
        shared_gate,
        shared_up,
        shared_down,
    )
    return layer((operands, shaped), local_experts, capacity, expert_ranks)


def solution(mesh):
    in_specs = (
        P("ep", "tp"),
        P("ep", "tp"),
        P("ep", "tp"),
        P(),
        P(),
        P("tp"),
        P("tp", None),
        P("ep", None),
        P(),
        P("ep", None),
        P("ep", None),
        P("ep", None, "tp"),
        P("ep", None, "tp"),
        P("ep", "tp", None),
        P(None, "tp"),
        P(None, "tp"),
        P("tp", None),
    )
    out_specs = (P(("ep", "tp"), None), P(("ep", "tp"), None))
    return jax.shard_map(shards, mesh=mesh, in_specs=in_specs, out_specs=out_specs, check_vma=False)
```

```python
import functools
import jax
import jax.numpy as jnp
from jax import lax
from jax.experimental import pallas as pl
from jax.experimental.pallas import tpu as pltpu
from jax.sharding import PartitionSpec as P

HEADS = 32
KV_HEADS = 8
HEAD_DIM = 64
WINDOW = 128
BLOCK = 128
TOP_K = 2


epsilon = 1e-06
masked_score = -1e30
score_scale = 0.125


def from_behind(block, axis, distance):
    devices = range(lax.axis_size(axis))
    route = [(i - distance, i) for i in devices if i - distance in devices]
    return lax.ppermute(block, axis, route)


def rms_scale(values, gain):
    widened = values.astype(jnp.float32)
    scaled = widened * lax.rsqrt(jnp.mean(widened * widened, axis=-1, keepdims=True) + epsilon)
    return (scaled * gain).astype(jnp.bfloat16)


def window_mask(first_block, block_count):
    query_pos = jnp.arange(BLOCK)[:, None]
    key_pos = jnp.arange(2 * BLOCK)[None, :]
    inside = (key_pos <= query_pos + BLOCK) & (key_pos > query_pos + BLOCK - WINDOW)
    not_first = (first_block + jnp.arange(block_count))[:, None, None] > 0
    return inside[None] & (not_first | (key_pos[None] >= BLOCK))


def band_blocks(rim_block, blocks_in):
    joined = jnp.concatenate([rim_block[None], blocks_in], axis=0)
    return jnp.concatenate([joined[:-1], joined[1:]], axis=1)


def layer_kernel(
    ranks,
    near,
    direct,
    order,
    program,
    local_experts,
    capacity,
    sink,
    query_hbm,
    key_hbm,
    value_hbm,
    query_gain,
    key_gain,
    out_hbm,
    tokens_hbm,
    gain_hbm,
    ids_hbm,
    route_hbm,
    gate_hbm,
    up_hbm,
    down_hbm,
    shared_gate_hbm,
    shared_up_hbm,
    shared_down_hbm,
    outputs,
    rows,
    kept,
    sibling_send,
    sibling_recv,
    peer_recv,
    far_out,
    near_out,
    far_back,
    near_back,
    mixer_part,
    shared_part,
    mixer_recv,
    shared_recv,
    mixer_send,
    mixer_peer,
    merged_send,
    merged_recv,
    total,
    tok,
    query,
    key_all,
    value_all,
    key_band,
    value_band,
    heads,
    ids,
    route,
    spots,
    picks,
    norm_gain,
    far_tok,
    far_ids,
    gate,
    up,
    down,
    out_weight,
    shared_gate,
    shared_up,
    shared_down,
    tok_sem,
    small_sem,
    weight_sem,
    rim_send,
    rim_recv,
    out_send,
    out_recv,
    fan_send,
    fan_recv,
    add_send,
    add_recv,
    back_send,
    back_recv,
    early_send,
    early_recv,
):
    rank = lax.axis_index("ep")
    part = lax.axis_index("tp")
    core = lax.rem(part, 2)
    side = part // 2
    sibling = 2 * side + 1 - core
    peer = 2 * (1 - side) + core
    across = 2 * (1 - side) + 1 - core
    placed = (part, peer, sibling, across)
    f32, bf16, i32 = jnp.float32, jnp.bfloat16, jnp.int32
    mesh_ids = pl.DeviceIdType.MESH
    width = rows.shape[-1]
    quarter = tok.shape[1]
    share = rows.shape[2]
    blocks = query.shape[0] // BLOCK
    pairs = query.shape[1] // 128
    spot_of = {k: s for s, k in enumerate(order)}
    chunk = 512
    chunks = width // chunk

    def partner(k):
        result = 0
        bit = 1
        while bit < ranks:
            own = lax.rem(rank // bit, 2)
            result = result + bit * ((1 - own) if k & bit else own)
            bit *= 2
        return result

    def send(source, target, send_sem, recv_sem, ep_to, tp_to):
        copy = pltpu.make_async_remote_copy(
            src_ref=source,
            dst_ref=target,
            send_sem=send_sem,
            recv_sem=recv_sem,
            device_id=(ep_to, tp_to),
            device_id_type=mesh_ids,
        )
        copy.start()
        sent.append(copy)
        return copy

    def arrive(copy):
        with jax.named_scope("wait"):
            copy.wait_recv()

    sent = []
    barrier = pltpu.get_barrier_semaphore()
    ahead = lax.rem(rank + 1, ranks)
    behind = lax.rem(rank + ranks - 1, ranks)
    for k in range(1, ranks):
        pl.semaphore_signal(barrier, inc=1, device_id=(partner(k), part), device_id_type=mesh_ids)
    for other in (sibling, peer):
        pl.semaphore_signal(barrier, inc=1, device_id=(rank, other), device_id_type=mesh_ids)

    def load(source, target, sem):
        copy = pltpu.make_async_copy(source, target, sem)
        copy.start()
        return copy

    def block_at(j):
        return pl.ds(pl.multiple_of(placed[j] * quarter, quarter), quarter)

    tok_loads = [load(tokens_hbm.at[block_at(j)], tok.at[j], tok_sem.at[j]) for j in range(4)]
    gain_load = load(gain_hbm, norm_gain, small_sem.at[0])
    id_loads = [load(ids_hbm.at[:, block_at(j)], ids.at[j], small_sem.at[1 + j]) for j in range(2)]
    sequence = query.shape[0]
    query_load = load(query_hbm, query, small_sem.at[5])
    key_load = load(key_hbm, key_all.at[pl.ds(BLOCK, sequence)], small_sem.at[6])
    value_load = load(value_hbm, value_all.at[pl.ds(BLOCK, sequence)], small_sem.at[7])
    route_loads = [
        load(route_hbm.at[:, block_at(j)], route.at[j], small_sem.at[3 + j]) for j in range(2)
    ]

    def norm_tokens(j):
        scoped("load", tok_loads[j].wait)
        wide = tok[j].astype(f32)
        scaled = wide * lax.rsqrt(jnp.mean(wide * wide, axis=-1, keepdims=True) + epsilon)
        tok[j] = (scaled * norm_gain[...]).astype(bf16)

    def bits(value, other):
        result = 0
        bit = 1
        while bit < ranks:
            own = lax.rem(other // bit, 2)
            theirs = lax.rem(value // bit, 2)
            result = result + bit * (theirs + own - 2 * theirs * own)
            bit *= 2
        return result

    def lay_out(named, source):
        experts_all = local_experts * ranks
        labels = lax.broadcasted_iota(i32, (experts_all, quarter), 0)
        behind_of = lax.broadcasted_iota(i32, (quarter, quarter), 0)
        below = (behind_of < lax.broadcasted_iota(i32, (quarter, quarter), 1)).astype(bf16)
        lines = [named[i : i + 1, :] for i in range(TOP_K)]
        hot = [(line == labels).astype(f32) for line in lines]
        before = jnp.dot(sum(hot).astype(bf16), below, preferred_element_type=f32)
        found = []
        for i, line in enumerate(lines):
            within = jnp.sum(hot[i] * before, axis=0, keepdims=True).astype(i32)
            ahead_of = bits(line // local_experts, source)
            found.append(ahead_of * share + lax.rem(line, local_experts) * capacity + within)
        return found

    def upright(line):
        return jnp.transpose(jnp.broadcast_to(line, (quarter, quarter)))[:, 0:1]

    def keep_layout(j, found):
        for i in range(TOP_K):
            spots[j, :, i : i + 1] = upright(found[i].astype(f32)).astype(i32)

    def keep_route():
        for j in range(2):
            route_loads[j].wait()
            for i in range(TOP_K):
                picks[j, :, i : i + 1] = upright(route[j, i : i + 1, :])

    def slot_rows(found, source, k, count):
        used = lax.broadcasted_iota(i32, (count * share, quarter), 0) + k * share
        chosen = sum((used == spot).astype(bf16) for spot in found)
        made = jnp.dot(chosen, source[...], preferred_element_type=f32)
        return made.astype(bf16).reshape(count, share, made.shape[1])

    dispatched = {}
    to_sibling = {}
    to_peer = {}
    relayed = {}
    added = {}
    peered = {}
    backs = {}

    def scoped(name, work, *settings):
        with jax.named_scope(name):
            return work(*settings)

    scoped("barrier", pl.semaphore_wait, barrier, ranks + 1)
    for copy in (key_load, value_load, *id_loads):
        copy.wait()
    rims = [
        send(
            held.at[pl.ds(sequence, BLOCK)],
            held.at[pl.ds(0, BLOCK)],
            rim_send.at[i],
            rim_recv.at[i],
            ahead,
            part,
        )
        for i, held in enumerate((key_all, value_all))
    ]
    names_sent = send(ids.at[0], far_ids, rim_send.at[2], rim_recv.at[2], partner(near), part)
    gain_load.wait()
    scoped("norm_0", norm_tokens, 0)
    weight_loads = [
        load(source, held, weight_sem.at[i])
        for i, (source, held) in enumerate(
            (
                (out_hbm, out_weight),
                (shared_gate_hbm, shared_gate),
                (shared_up_hbm, shared_up),
                (shared_down_hbm, shared_down),
                (gate_hbm, gate),
                (up_hbm, up),
                (down_hbm, down),
            )
        )
    ]
    found_own = scoped("lay_out_0", lay_out, ids[0], rank)
    scoped("norm_1", norm_tokens, 1)
    found_peer = scoped("lay_out_1", lay_out, ids[1], rank)

    def give(n, source, target, h):
        return send(
            source,
            target,
            out_send.at[h, n],
            out_recv.at[h, n],
            partner(n if n < near else n - near),
            part,
        )

    halves = [pl.ds(h * (width // 2), width // 2) for h in range(2)]
    for n in range(1, near):
        near_out[n - 1, 0:1] = scoped("near_rows", slot_rows, found_own, tok.at[0], n, 1)
        if n < direct:
            near_out[n - 1, 1:2] = scoped("near_rows", slot_rows, found_peer, tok.at[1], n, 1)
            dispatched[n] = [give(n, near_out.at[n - 1], rows.at[spot_of[n], pl.ds(0, 2)], 0)]
        else:
            dispatched[n] = [give(n, near_out.at[n - 1, 0], rows.at[spot_of[n], 0], 0)]
        if n == 1:
            dense_sent = [
                send(
                    tok.at[0, :, columns],
                    far_tok.at[:, columns],
                    out_send.at[h, near],
                    out_recv.at[h, near],
                    partner(near),
                    part,
                )
                for h, columns in enumerate(halves)
            ]
    rows[spot_of[0], 0:1] = scoped("rows", slot_rows, found_own, tok.at[0], 0, 1)
    rows[spot_of[0], 1:2] = scoped("rows", slot_rows, found_peer, tok.at[1], 0, 1)

    def proxy(h):
        columns = halves[h]
        if h == 0:
            arrive(names_sent)
        arrive(dense_sent[h])
        found = lay_out(far_ids[...], partner(near))
        s = spot_of[near]
        source = far_tok.at[:, columns]
        rows[s, 0:1, :, columns] = slot_rows(found, source, near, 1)
        own = rows.at[s, 0, :, columns]
        to_peer.setdefault(near, []).append(
            send(
                own,
                rows.at[s, 1, :, columns],
                fan_send.at[3 * h, near],
                fan_recv.at[3 * h, near],
                rank,
                peer,
            )
        )
        to_sibling.setdefault(near, []).append(
            send(
                own,
                rows.at[s, 2, :, columns],
                fan_send.at[1 + 3 * h, near],
                fan_recv.at[1 + 3 * h, near],
                rank,
                sibling,
            )
        )
        for n in range(near + 1, ranks):
            far_out[n - near - 1, :, columns] = slot_rows(found, source, n, 1)[0]
            dispatched.setdefault(n, []).append(
                give(
                    n,
                    far_out.at[n - near - 1, :, columns],
                    rows.at[spot_of[n], 0, :, columns],
                    h,
                )
            )

    def layouts():
        keep_layout(0, found_own)
        keep_layout(1, found_peer)
        keep_route()

    low = lax.broadcasted_iota(i32, (BLOCK, 128), 1) < HEAD_DIM

    def head_scale(values, gain):
        squares = values * values
        lower = jnp.sum(jnp.where(low, squares, 0.0), axis=1, keepdims=True)
        upper = jnp.sum(jnp.where(low, 0.0, squares), axis=1, keepdims=True)
        mean = jnp.where(low, lower, upper) * (1.0 / HEAD_DIM)
        return values * lax.rsqrt(mean + epsilon) * gain

    def doubled(gain):
        return jnp.concatenate([gain[...], gain[...]], axis=1)

    def band_block(index, carry):
        at = pl.ds(pl.multiple_of(index * BLOCK, BLOCK), BLOCK)
        keys = head_scale(key_all[at].astype(f32), doubled(key_gain))
        values = value_all[at].astype(f32)
        for wide, band in ((keys, key_band), (values, value_band)):
            turned = pltpu.roll(wide, HEAD_DIM, 1)
            band[0, 0, at] = jnp.where(low, wide, 0.0).astype(bf16)
            band[0, 1, at] = jnp.where(low, 0.0, turned).astype(bf16)
            band[1, 0, at] = jnp.where(low, turned, 0.0).astype(bf16)
            band[1, 1, at] = jnp.where(low, 0.0, wide).astype(bf16)
        return carry

    def attend(n, slot):
        at = pl.ds(pl.multiple_of(n * BLOCK, BLOCK), BLOCK)
        span = pl.ds(pl.multiple_of(n * BLOCK, BLOCK), 2 * BLOCK)
        query_pos = lax.broadcasted_iota(i32, (BLOCK, 2 * BLOCK), 0)
        key_pos = lax.broadcasted_iota(i32, (BLOCK, 2 * BLOCK), 1)
        floor = jnp.where(rank * blocks + n > 0, 0, BLOCK)
        inside = (key_pos <= query_pos + BLOCK) & (key_pos > query_pos + BLOCK - WINDOW)
        inside = inside & (key_pos >= floor)
        for pair in range(pairs):
            kv = pair * 2 // (HEADS // KV_HEADS)
            lanes = slice(pair * 128, pair * 128 + 128)
            normed = head_scale(query[at, lanes].astype(f32), doubled(query_gain)).astype(bf16)
            keys = key_band[kv, :, span].reshape(4 * BLOCK, 128)
            scores = lax.dot_general(
                normed, keys, (((1,), (1,)), ((), ())), preferred_element_type=f32
            )
            probs = []
            for h in range(2):
                logit = sink[2 * pair + h]
                score = scores[:, h * 2 * BLOCK : (h + 1) * 2 * BLOCK] * score_scale
                score = jnp.where(inside, score, masked_score)
                top = jnp.maximum(jnp.max(score, axis=1, keepdims=True), logit)
                raised = jnp.exp(score - top)
                below = jnp.sum(raised, axis=1, keepdims=True) + jnp.exp(logit - top)
                probs.append((raised * (1.0 / below)).astype(bf16))
            values = value_band[kv, :, span].reshape(4 * BLOCK, 128)
            made = jnp.dot(jnp.concatenate(probs, axis=1), values, preferred_element_type=f32)
            heads[slot, :, lanes] = made.astype(bf16)

    def keys():
        query_load.wait()
        lax.fori_loop(1, blocks + 1, band_block, 0)
        for rim in rims:
            arrive(rim)
        band_block(0, 0)

    def attend_half(half):
        def one(step, carry):
            j = 2 * step + half
            n = 2 * (side + half - 2 * side * half) + core + step - 2 * core * step
            attend(n, j)
            return carry

        lax.fori_loop(0, 2, one, 0)

    def early_pair(i, full, received):
        return send(
            full.at[pl.ds(2, 2)], received, early_send.at[i], early_recv.at[i], rank, sibling
        )

    early = {}

    def mixer(half):
        if half:
            weight_loads[0].wait()
        held = jnp.concatenate([heads[half], heads[2 + half]], axis=0)

        def one(c, carry):
            at = pl.ds(pl.multiple_of(c * chunk, chunk), chunk)
            made = jnp.dot(held, out_weight[:, at], preferred_element_type=f32).astype(bf16)
            mixer_part[half, :, at] = made[:quarter]
            mixer_part[2 + half, :, at] = made[quarter:]
            return carry

        lax.fori_loop(0, chunks, one, 0)
        early["mixer", half] = send(
            mixer_part.at[2 + half],
            mixer_recv.at[half],
            early_send.at[4 * half],
            early_recv.at[4 * half],
            rank,
            sibling,
        )

    def shared():
        for i in (1, 2, 3):
            weight_loads[i].wait()
        for half in (1, 0):
            held = tok[2 * half : 2 * half + 2].reshape(2 * quarter, width)
            gate_part = jnp.dot(held, shared_gate[...], preferred_element_type=f32)
            up_part = jnp.dot(held, shared_up[...], preferred_element_type=f32)
            hidden = (gate_part / (1.0 + jnp.exp(-gate_part)) * up_part).astype(bf16)

            def one(c, carry):
                at = pl.ds(pl.multiple_of(c * chunk, chunk), chunk)
                made = jnp.dot(hidden, shared_down[:, at], preferred_element_type=f32)
                shared_part[2 * half : 2 * half + 2, :, at] = made.astype(bf16).reshape(
                    2, quarter, chunk
                )
                return carry

            lax.fori_loop(0, chunks, one, 0)
            if half:
                early["shared"] = early_pair(1, shared_part, shared_recv)

    def mixer_add():
        arrive(early["mixer", 1])
        mixer_send[...] = (mixer_part[1].astype(f32) + mixer_recv[1].astype(f32)).astype(bf16)
        early["peer"] = send(
            mixer_send, mixer_peer, early_send.at[2], early_recv.at[2], rank, peer
        )

    def mixer_finish():
        arrive(early["mixer", 0])
        arrive(early["peer"])
        outputs[0] = (
            mixer_part[0].astype(f32) + mixer_recv[0].astype(f32) + mixer_peer[...].astype(f32)
        ).astype(bf16)

    def pass_on(k, sem, which, count):
        s = spot_of[k]
        return send(
            rows.at[s, pl.ds(which, count)],
            rows.at[s, pl.ds(2 + which, count)],
            fan_send.at[sem, k],
            fan_recv.at[sem, k],
            rank,
            sibling,
        )

    def fan(k):
        s = spot_of[k]
        for copy in dispatched.get(k, ()):
            arrive(copy)
        if k >= direct:
            to_peer[k] = [
                send(
                    rows.at[s, 0], rows.at[s, 1], fan_send.at[0, k], fan_recv.at[0, k], rank, peer
                )
            ]
            to_sibling[k] = [pass_on(k, 1, 0, 1)]
        else:
            to_sibling[k] = [pass_on(k, 1, 0, 2)]

    def relay(k):
        for copy in to_peer[k]:
            arrive(copy)
        relayed[k] = pass_on(k, 2, 1, 1)

    ready = []

    def experts(*names):
        count = len(names)
        first = spot_of[names[0]]
        for k in names:
            for copy in to_sibling[k]:
                arrive(copy)
            if k in relayed:
                arrive(relayed[k])
        if not ready:
            for i in (4, 5, 6):
                weight_loads[i].wait()
            ready.append(True)

        def one(index, carry):
            at = pl.ds(pl.multiple_of(index * capacity, capacity), capacity)
            block = rows[first : first + count, :, at, :].reshape(count * 4 * capacity, width)
            gate_part = jnp.dot(block, gate[index], preferred_element_type=f32)
            up_part = jnp.dot(block, up[index], preferred_element_type=f32)
            hidden = (gate_part / (1.0 + jnp.exp(-gate_part)) * up_part).astype(bf16)
            made = jnp.dot(hidden, down[index], preferred_element_type=f32)
            made = made.astype(bf16).reshape(count, 4, capacity, width)
            spot = pl.ds(first, count)
            kept[spot, :, at, :] = made[:, 0:2]
            sibling_send[spot, :, at, :] = made[:, 2:4]
            return carry

        lax.fori_loop(0, local_experts, one, 0)
        for k in names:
            s = spot_of[k]
            added[k] = send(
                sibling_send.at[s],
                sibling_recv.at[s],
                add_send.at[0, k],
                add_recv.at[0, k],
                rank,
                sibling,
            )

    def add_pair(k):
        s = spot_of[k]
        arrive(added[k])
        if k >= near:
            for h, columns in enumerate(halves):
                kept[s, 1, :, columns] = (
                    kept[s, 1, :, columns].astype(f32) + sibling_recv[s, 1, :, columns].astype(f32)
                ).astype(bf16)
                peered[k, h] = send(
                    kept.at[s, 1, :, columns],
                    peer_recv.at[k - near, :, columns],
                    add_send.at[1 + h, k],
                    add_recv.at[1 + h, k],
                    rank,
                    peer,
                )
            return
        both = (kept[s].astype(f32) + sibling_recv[s].astype(f32)).astype(bf16)
        if k == 0:
            near_back[0] = both
            return
        kept[s] = both

    def give_back(k):
        backs[k] = send(
            kept.at[spot_of[k]],
            near_back.at[k],
            back_send.at[0, k],
            back_recv.at[0, k],
            partner(k),
            part,
        )

    def finish(k, h):
        s = spot_of[k]
        columns = halves[h]
        arrive(peered[k, h])
        kept[s, 0, :, columns] = (
            kept[s, 0, :, columns].astype(f32)
            + sibling_recv[s, 0, :, columns].astype(f32)
            + peer_recv[k - near, :, columns].astype(f32)
        ).astype(bf16)
        backs[k, h] = send(
            kept.at[s, 0, :, columns],
            far_back.at[k - near, :, columns],
            back_send.at[h, k],
            back_recv.at[h, k],
            partner(k),
            part,
        )

    def picked(j, source, first):
        count = source.shape[0]
        slots = lax.broadcasted_iota(i32, (quarter, count), 1) + first
        result = 0
        for i in range(TOP_K):
            hot = (spots[j, :, i : i + 1] == slots).astype(bf16)
            result = result + jnp.dot(hot, source, preferred_element_type=f32) * picks[
                j, :, i : i + 1
            ]
        return result

    def near_sum(j):
        if j:
            for k in range(1, near):
                arrive(backs[k])
            arrive(early["shared"])

        def one(c, carry):
            at = pl.ds(pl.multiple_of(c * chunk, chunk), chunk)
            source = near_back[:, j, :, at].reshape(near * share, chunk)
            value = (
                shared_part[j, :, at].astype(f32)
                + shared_recv[j, :, at].astype(f32)
                + picked(j, source, 0)
            )
            if j:
                merged_send[:, at] = value.astype(bf16)
            else:
                total[:, at] = value
            return carry

        lax.fori_loop(0, chunks, one, 0)
        if j:
            early["merged"] = send(
                merged_send, merged_recv, early_send.at[3], early_recv.at[3], rank, peer
            )

    def far_sum(first, count):
        last = first + count == ranks
        for k in range(first, first + count):
            for h in range(2):
                arrive(backs[k, h])
        if last:
            arrive(early["merged"])

        def one(c, carry):
            at = pl.ds(pl.multiple_of(c * chunk, chunk), chunk)
            source = far_back[first - near : first - near + count, :, at].reshape(
                count * share, chunk
            )
            value = total[:, at] + picked(0, source, first * share)
            if last:
                value = value + merged_recv[:, at].astype(f32)
                outputs[1, :, at] = value.astype(bf16)
            else:
                total[:, at] = value
            return carry

        lax.fori_loop(0, chunks, one, 0)

    steps = {
        "proxy": proxy,
        "layouts": layouts,
        "norm": norm_tokens,
        "keys": keys,
        "attend": attend_half,
        "mixer": mixer,
        "shared": shared,
        "mixer_add": mixer_add,
        "mixer_finish": mixer_finish,
        "fan": fan,
        "relay": relay,
        "experts": experts,
        "add": add_pair,
        "back": give_back,
        "finish": finish,
        "near_sum": near_sum,
        "far_sum": far_sum,
    }
    for name, *settings in program:
        with jax.named_scope("_".join(map(str, (name, *settings)))):
            steps[name](*settings)
    for copy in sent:
        copy.wait_send()


def step_order(direct):
    program = (
        ("keys",), ("attend", 1), ("attend", 0), ("mixer", 1), ("mixer", 0), ("mixer_add",),
        ("proxy", 0), ("proxy", 1), ("fan", 3), ("fan", 0), ("relay", 4), ("experts", 4),
        ("fan", 5), ("fan", 2), ("relay", 3), ("experts", 2, 3), ("fan", 1), ("relay", 5),
        ("add", 4), ("fan", 6), ("add", 3), ("back", 3), ("experts", 5), ("finish", 4, 0),
        ("finish", 4, 1), ("add", 5), ("experts", 0, 1), ("add", 1), ("layouts",),
        ("mixer_finish",), ("norm", 3), ("relay", 6), ("finish", 5, 0), ("finish", 5, 1),
        ("fan", 7), ("experts", 6), ("back", 1), ("add", 2), ("back", 2), ("add", 6),
        ("relay", 7), ("norm", 2), ("finish", 6, 0), ("finish", 6, 1), ("experts", 7),
        ("shared",), ("add", 7), ("add", 0), ("near_sum", 1), ("finish", 7, 0),
        ("finish", 7, 1), ("near_sum", 0), ("far_sum", 4, 2), ("far_sum", 6, 1),
        ("far_sum", 7, 1),
    )
    return [step for step in program if step[0] != "relay" or step[1] >= direct]


def layer(arrays, local_experts, capacity, ranks):
    query_rows, out_weight, tokens, gate, up, down, shared_gate, shared_up, shared_down = arrays[1]
    near, direct = 4, 3
    order = tuple(range(ranks))
    bf16, f32 = jnp.bfloat16, jnp.float32
    dma = pltpu.SemaphoreType.DMA
    quarter = tokens.shape[0] // 4
    width = tokens.shape[1]
    share = local_experts * capacity
    sequence = query_rows.shape[0]
    far = ranks - near
    vmem = pl.BlockSpec(memory_space=pltpu.VMEM)
    anywhere = pl.BlockSpec(memory_space=pl.ANY)
    smem = pl.BlockSpec(memory_space=pltpu.SMEM)

    def held(*shape):
        return pltpu.VMEM(shape, bf16)

    return pl.pallas_call(
        functools.partial(
            layer_kernel, ranks, near, direct, order, step_order(direct), local_experts, capacity
        ),
        out_shape=jax.ShapeDtypeStruct((2, quarter, width), bf16),
        in_specs=[smem]
        + [anywhere] * 3
        + [vmem] * 2
        + [anywhere] * 11,
        out_specs=vmem,
        scratch_shapes=[
            held(ranks, 4, share, width),
            held(ranks, 2, share, width),
            held(ranks, 2, share, width),
            held(ranks, 2, share, width),
            held(far, share, width),
            held(far - 1, share, width),
            held(near - 1, 2, share, width),
            held(far, share, width),
            held(near, 2, share, width),
            held(4, quarter, width),
            held(4, quarter, width),
            held(2, quarter, width),
            held(2, quarter, width),
            held(quarter, width),
            held(quarter, width),
            held(quarter, width),
            held(quarter, width),
            pltpu.VMEM((quarter, width), f32),
            held(4, quarter, width),
            held(*query_rows.shape),
            held(sequence + BLOCK, 128),
            held(sequence + BLOCK, 128),
            held(2, 2, sequence + BLOCK, 128),
            held(2, 2, sequence + BLOCK, 128),
            held(4, quarter, query_rows.shape[1]),
            pltpu.VMEM((2, TOP_K, quarter), jnp.int32),
            pltpu.VMEM((2, TOP_K, quarter), f32),
            pltpu.VMEM((2, quarter, TOP_K), jnp.int32),
            pltpu.VMEM((2, quarter, TOP_K), f32),
            pltpu.VMEM((1, width), f32),
            held(quarter, width),
            pltpu.VMEM((TOP_K, quarter), jnp.int32),
            held(*gate.shape),
            held(*up.shape),
            held(*down.shape),
            held(*out_weight.shape),
            held(*shared_gate.shape),
            held(*shared_up.shape),
            held(*shared_down.shape),
            dma((4,)),
            dma((8,)),
            dma((7,)),
            dma((3,)),
            dma((3,)),
            dma((2, ranks)),
            dma((2, ranks)),
            dma((5, ranks)),
            dma((5, ranks)),
            dma((3, ranks)),
            dma((3, ranks)),
            dma((2, ranks)),
            dma((2, ranks)),
            dma((5,)),
            dma((5,)),
        ],
        compiler_params=pltpu.CompilerParams(
            collective_id=0, has_side_effects=True, vmem_limit_bytes=65000 * 1024
        ),
    )(*arrays[0])


def wide_shards(
    query_rows,
    key_rows,
    value_rows,
    query_gain,
    key_gain,
    sink_logit,
    out_weight,
    tokens,
    norm_gain,
    expert_ids,
    route_weight,
    gate_weight,
    up_weight,
    down_weight,
    shared_gate,
    shared_up,
    shared_down,
):
    expert_ranks = lax.axis_size("ep")
    head_ranks = lax.axis_size("tp")
    head_rank = lax.axis_index("tp")
    sequence_rows = query_rows.shape[0]
    blocks = sequence_rows // BLOCK
    pair_heads = key_rows.shape[1] // HEAD_DIM
    group_size = HEADS // KV_HEADS
    query_normed = rms_scale(
        query_rows.reshape(blocks, BLOCK, pair_heads, group_size, HEAD_DIM), query_gain
    )
    key_normed = rms_scale(key_rows.reshape(blocks, BLOCK, pair_heads, HEAD_DIM), key_gain)
    value_blocks = value_rows.reshape(blocks, BLOCK, pair_heads, HEAD_DIM)
    rim_keys, rim_values = from_behind((key_normed[blocks - 1], value_blocks[blocks - 1]), "ep", 1)
    key_band = band_blocks(rim_keys, key_normed)
    value_band = band_blocks(rim_values, value_blocks)
    window = window_mask(lax.axis_index("ep") * blocks, blocks)
    scores = (
        jnp.einsum("nqhgd,nkhd->hgnqk", query_normed, key_band, preferred_element_type=jnp.float32)
        * score_scale
    )
    scores = jnp.where(window[None, None], scores, masked_score)
    sink_col = sink_logit.reshape(pair_heads, group_size, 1, 1, 1)
    row_max = jnp.maximum(jnp.max(scores, axis=-1, keepdims=True), sink_col)
    exp_scores = jnp.exp(scores - row_max)
    attn_probs = (
        exp_scores / (jnp.sum(exp_scores, axis=-1, keepdims=True) + jnp.exp(sink_col - row_max))
    ).astype(jnp.bfloat16)
    heads_out = (
        jnp.einsum("hgnqk,nkhd->nqhgd", attn_probs, value_band, preferred_element_type=jnp.float32)
        .astype(jnp.bfloat16)
        .reshape(sequence_rows, pair_heads * group_size * HEAD_DIM)
    )
    local_experts = gate_weight.shape[0]
    expert_total = local_experts * expert_ranks
    quarter = tokens.shape[0] // head_ranks
    model_width = tokens.shape[1]
    capacity = 2 * quarter * TOP_K // expert_total
    slot_share = local_experts * capacity
    routed_rows = expert_ranks * slot_share
    normed = rms_scale(tokens, norm_gain)
    route_ids = expert_ids.reshape(head_ranks, quarter * TOP_K)
    one_hot = (route_ids[:, :, None] == jnp.arange(expert_total, dtype=jnp.int32)).astype(jnp.int32)
    slot_rank = jnp.sum(one_hot * (jnp.cumsum(one_hot, axis=1) - 1), axis=-1)
    positions = route_ids * capacity + slot_rank
    owners = jnp.arange(quarter * TOP_K, dtype=jnp.int32) // TOP_K
    padded_rows = jnp.concatenate(
        [
            normed.reshape(head_ranks, quarter, model_width),
            jnp.zeros((head_ranks, 1, model_width), jnp.bfloat16),
        ],
        axis=1,
    ).reshape(head_ranks * (quarter + 1), model_width)
    slot_token = (
        jnp.full((head_ranks, routed_rows), quarter, jnp.int32)
        .at[jnp.arange(head_ranks, dtype=jnp.int32)[:, None], positions]
        .set(jnp.broadcast_to(owners[None, :], positions.shape))
    )
    slot_index = slot_token + (jnp.arange(head_ranks, dtype=jnp.int32) * (quarter + 1))[:, None]
    own_index = lax.dynamic_index_in_dim(slot_index, head_rank, 0, keepdims=True)
    outgoing = padded_rows[own_index].reshape(1, expert_ranks, slot_share, model_width)
    arrived = lax.all_to_all(outgoing, "ep", split_axis=1, concat_axis=1, tiled=True)
    piece_rows = lax.all_gather(
        arrived.reshape(1, expert_ranks, local_experts, capacity, model_width),
        "tp",
        axis=0,
        tiled=True,
    )
    gate_part = jnp.einsum(
        "tsecd,edf->tsecf", piece_rows, gate_weight, preferred_element_type=jnp.float32
    )
    up_part = jnp.einsum(
        "tsecd,edf->tsecf", piece_rows, up_weight, preferred_element_type=jnp.float32
    )
    hidden = (jax.nn.silu(gate_part) * up_part).astype(jnp.bfloat16)
    shared_hidden = (
        jax.nn.silu(jnp.dot(normed, shared_gate, preferred_element_type=jnp.float32))
        * jnp.dot(normed, shared_up, preferred_element_type=jnp.float32)
    ).astype(jnp.bfloat16)
    span_rows = routed_rows + quarter
    mixer_out = lax.psum_scatter(
        jnp.dot(heads_out, out_weight, preferred_element_type=jnp.float32).astype(jnp.bfloat16),
        "tp",
        scatter_dimension=0,
        tiled=True,
    )
    part_count = lax.axis_size("tp") * span_rows // span_rows
    routed_part = jnp.einsum(
        "tsecf,efd->tsecd", hidden, down_weight, preferred_element_type=jnp.float32
    ).reshape(part_count, routed_rows, model_width)
    shared_part = jnp.dot(shared_hidden, shared_down, preferred_element_type=jnp.float32).reshape(
        part_count, quarter, model_width
    )
    summed = lax.psum_scatter(
        jnp.concatenate([routed_part, shared_part], axis=1)
        .reshape(part_count * span_rows, model_width)
        .astype(jnp.bfloat16),
        "tp",
        scatter_dimension=0,
        tiled=True,
    )
    returned = lax.all_to_all(
        summed[:routed_rows].reshape(expert_ranks, slot_share, model_width),
        "ep",
        split_axis=0,
        concat_axis=0,
        tiled=True,
    ).reshape(routed_rows, model_width)
    own_positions = lax.dynamic_index_in_dim(positions, head_rank, 0, keepdims=False)
    picked = returned[own_positions].reshape(quarter, TOP_K, model_width).astype(jnp.float32)
    own_weights = lax.dynamic_slice_in_dim(route_weight, head_rank * quarter, quarter, 0)
    expert_out = (
        summed[routed_rows:].astype(jnp.float32) + jnp.sum(picked * own_weights[:, :, None], axis=1)
    ).astype(jnp.bfloat16)
    return (mixer_out, expert_out)


def shards(
    query_rows,
    key_rows,
    value_rows,
    query_gain,
    key_gain,
    sink_logit,
    out_weight,
    tokens,
    norm_gain,
    expert_ids,
    route_weight,
    gate_weight,
    up_weight,
    down_weight,
    shared_gate,
    shared_up,
    shared_down,
):
    expert_ranks = lax.axis_size("ep")
    head_ranks = lax.axis_size("tp")
    local_experts = gate_weight.shape[0]
    expert_total = local_experts * expert_ranks
    quarter = tokens.shape[0] // head_ranks
    capacity = 2 * quarter * TOP_K // expert_total
    fits = (
        head_ranks == 4
        and expert_ranks == 8
        and capacity % 16 == 0
        and quarter == BLOCK
        and query_rows.shape[0] == 4 * BLOCK
        and key_rows.shape[1] == 2 * HEAD_DIM
    )
    if not fits:
        return wide_shards(
            query_rows,
            key_rows,
            value_rows,
            query_gain,
            key_gain,
            sink_logit,
            out_weight,
            tokens,
            norm_gain,
            expert_ids,
            route_weight,
            gate_weight,
            up_weight,
            down_weight,
            shared_gate,
            shared_up,
            shared_down,
        )
    operands = (
        sink_logit,
        query_rows,
        key_rows,
        value_rows,
        query_gain.reshape(1, HEAD_DIM),
        key_gain.reshape(1, HEAD_DIM),
        out_weight,
        tokens,
        norm_gain.reshape(1, tokens.shape[1]),
        expert_ids.T,
        route_weight.T,
        gate_weight,
        up_weight,
        down_weight,
        shared_gate,
        shared_up,
        shared_down,
    )
    shaped = (
        query_rows,
        out_weight,
        tokens,
        gate_weight,
        up_weight,
        down_weight,
        shared_gate,
        shared_up,
        shared_down,
    )
    both = layer((operands, shaped), local_experts, capacity, expert_ranks)
    return both[0], both[1]


def solution(mesh):
    in_specs = (
        P("ep", "tp"),
        P("ep", "tp"),
        P("ep", "tp"),
        P(),
        P(),
        P("tp"),
        P("tp", None),
        P("ep", None),
        P(),
        P("ep", None),
        P("ep", None),
        P("ep", None, "tp"),
        P("ep", None, "tp"),
        P("ep", "tp", None),
        P(None, "tp"),
        P(None, "tp"),
        P("tp", None),
    )
    out_specs = (P(("ep", "tp"), None), P(("ep", "tp"), None))
    return jax.shard_map(shards, mesh=mesh, in_specs=in_specs, out_specs=out_specs, check_vma=False)
```

```python
import functools
import jax
import jax.numpy as jnp
from jax import lax
from jax.experimental import pallas as pl
from jax.experimental.pallas import tpu as pltpu
from jax.sharding import PartitionSpec as P

HEADS = 32
KV_HEADS = 8
HEAD_DIM = 64
WINDOW = 128
BLOCK = 128
TOP_K = 2


epsilon = 1e-06
masked_score = -1e30
score_scale = 0.125


def from_behind(block, axis, distance):
    devices = range(lax.axis_size(axis))
    route = [(i - distance, i) for i in devices if i - distance in devices]
    return lax.ppermute(block, axis, route)


def rms_scale(values, gain):
    widened = values.astype(jnp.float32)
    scaled = widened * lax.rsqrt(jnp.mean(widened * widened, axis=-1, keepdims=True) + epsilon)
    return (scaled * gain).astype(jnp.bfloat16)


def window_mask(first_block, block_count):
    query_pos = jnp.arange(BLOCK)[:, None]
    key_pos = jnp.arange(2 * BLOCK)[None, :]
    inside = (key_pos <= query_pos + BLOCK) & (key_pos > query_pos + BLOCK - WINDOW)
    not_first = (first_block + jnp.arange(block_count))[:, None, None] > 0
    return inside[None] & (not_first | (key_pos[None] >= BLOCK))


def band_blocks(rim_block, blocks_in):
    joined = jnp.concatenate([rim_block[None], blocks_in], axis=0)
    return jnp.concatenate([joined[:-1], joined[1:]], axis=1)


def layer_kernel(
    ranks,
    near,
    direct,
    order,
    program,
    local_experts,
    capacity,
    sink,
    query_hbm,
    key_hbm,
    value_hbm,
    query_gain,
    key_gain,
    out_hbm,
    tokens_hbm,
    gain_hbm,
    ids_hbm,
    route_hbm,
    gate_hbm,
    up_hbm,
    down_hbm,
    shared_gate_hbm,
    shared_up_hbm,
    shared_down_hbm,
    outputs,
    results,
    flush_sem,
    rows,
    kept,
    sibling_send,
    sibling_recv,
    peer_recv,
    far_out,
    near_out,
    far_back,
    near_back,
    mixer_part,
    shared_part,
    mixer_recv,
    shared_recv,
    mixer_send,
    mixer_peer,
    merged_send,
    merged_recv,
    total,
    tok,
    query,
    key_all,
    value_all,
    key_band,
    value_band,
    heads,
    ids,
    route,
    spots,
    picks,
    norm_gain,
    far_tok,
    far_ids,
    gate,
    up,
    down,
    out_weight,
    shared_gate,
    shared_up,
    shared_down,
    tok_sem,
    small_sem,
    weight_sem,
    rim_send,
    rim_recv,
    out_send,
    out_recv,
    fan_send,
    fan_recv,
    add_send,
    add_recv,
    back_send,
    back_recv,
    early_send,
    early_recv,
):
    rank = lax.axis_index("ep")
    part = lax.axis_index("tp")
    core = lax.rem(part, 2)
    side = part // 2
    sibling = 2 * side + 1 - core
    peer = 2 * (1 - side) + core
    across = 2 * (1 - side) + 1 - core
    placed = (part, peer, sibling, across)
    f32, bf16, i32 = jnp.float32, jnp.bfloat16, jnp.int32
    mesh_ids = pl.DeviceIdType.MESH
    width = rows.shape[-1]
    quarter = tok.shape[1]
    share = rows.shape[2]
    blocks = query.shape[0] // BLOCK
    pairs = query.shape[1] // 128
    spot_of = {k: s for s, k in enumerate(order)}
    chunk = 512
    chunks = width // chunk

    def partner(k):
        result = 0
        bit = 1
        while bit < ranks:
            own = lax.rem(rank // bit, 2)
            result = result + bit * ((1 - own) if k & bit else own)
            bit *= 2
        return result

    def send(source, target, send_sem, recv_sem, ep_to, tp_to):
        copy = pltpu.make_async_remote_copy(
            src_ref=source,
            dst_ref=target,
            send_sem=send_sem,
            recv_sem=recv_sem,
            device_id=(ep_to, tp_to),
            device_id_type=mesh_ids,
        )
        copy.start()
        sent.append(copy)
        return copy

    def arrive(copy):
        with jax.named_scope("wait"):
            copy.wait_recv()

    sent = []
    barrier = pltpu.get_barrier_semaphore()
    ahead = lax.rem(rank + 1, ranks)
    behind = lax.rem(rank + ranks - 1, ranks)
    for k in range(1, ranks):
        pl.semaphore_signal(barrier, inc=1, device_id=(partner(k), part), device_id_type=mesh_ids)
    for other in (sibling, peer):
        pl.semaphore_signal(barrier, inc=1, device_id=(rank, other), device_id_type=mesh_ids)

    def load(source, target, sem):
        copy = pltpu.make_async_copy(source, target, sem)
        copy.start()
        return copy

    def block_at(j):
        return pl.ds(pl.multiple_of(placed[j] * quarter, quarter), quarter)

    tok_loads = [load(tokens_hbm.at[block_at(j)], tok.at[j], tok_sem.at[j]) for j in range(4)]
    gain_load = load(gain_hbm, norm_gain, small_sem.at[0])
    id_loads = [load(ids_hbm.at[:, block_at(j)], ids.at[j], small_sem.at[1 + j]) for j in range(2)]
    sequence = query.shape[0]
    query_load = load(query_hbm, query, small_sem.at[5])
    key_load = load(key_hbm, key_all.at[pl.ds(BLOCK, sequence)], small_sem.at[6])
    value_load = load(value_hbm, value_all.at[pl.ds(BLOCK, sequence)], small_sem.at[7])
    route_loads = [
        load(route_hbm.at[:, block_at(j)], route.at[j], small_sem.at[3 + j]) for j in range(2)
    ]

    def norm_tokens(j):
        scoped("load", tok_loads[j].wait)
        wide = tok[j].astype(f32)
        scaled = wide * lax.rsqrt(jnp.mean(wide * wide, axis=-1, keepdims=True) + epsilon)
        tok[j] = (scaled * norm_gain[...]).astype(bf16)

    def bits(value, other):
        result = 0
        bit = 1
        while bit < ranks:
            own = lax.rem(other // bit, 2)
            theirs = lax.rem(value // bit, 2)
            result = result + bit * (theirs + own - 2 * theirs * own)
            bit *= 2
        return result

    def lay_out(named, source):
        experts_all = local_experts * ranks
        labels = lax.broadcasted_iota(i32, (experts_all, quarter), 0)
        behind_of = lax.broadcasted_iota(i32, (quarter, quarter), 0)
        below = (behind_of < lax.broadcasted_iota(i32, (quarter, quarter), 1)).astype(bf16)
        lines = [named[i : i + 1, :] for i in range(TOP_K)]
        hot = [(line == labels).astype(f32) for line in lines]
        before = jnp.dot(sum(hot).astype(bf16), below, preferred_element_type=f32)
        found = []
        for i, line in enumerate(lines):
            within = jnp.sum(hot[i] * before, axis=0, keepdims=True).astype(i32)
            ahead_of = bits(line // local_experts, source)
            found.append(ahead_of * share + lax.rem(line, local_experts) * capacity + within)
        return found

    def upright(line):
        return jnp.transpose(jnp.broadcast_to(line, (quarter, quarter)))[:, 0:1]

    def keep_layout(j, found):
        for i in range(TOP_K):
            spots[j, :, i : i + 1] = upright(found[i].astype(f32)).astype(i32)

    def keep_route():
        for j in range(2):
            route_loads[j].wait()
            for i in range(TOP_K):
                picks[j, :, i : i + 1] = upright(route[j, i : i + 1, :])

    def slot_rows(found, source, k, count):
        used = lax.broadcasted_iota(i32, (count * share, quarter), 0) + k * share
        chosen = sum((used == spot).astype(bf16) for spot in found)
        made = jnp.dot(chosen, source[...], preferred_element_type=f32)
        return made.astype(bf16).reshape(count, share, width)

    dispatched = {}
    to_sibling = {}
    to_peer = {}
    relayed = {}
    added = {}
    peered = {}
    backs = {}

    def scoped(name, work, *settings):
        with jax.named_scope(name):
            return work(*settings)

    scoped("barrier", pl.semaphore_wait, barrier, ranks + 1)
    for copy in (key_load, value_load, *id_loads):
        copy.wait()
    rims = [
        send(
            held.at[pl.ds(sequence, BLOCK)],
            held.at[pl.ds(0, BLOCK)],
            rim_send.at[i],
            rim_recv.at[i],
            ahead,
            part,
        )
        for i, held in enumerate((key_all, value_all))
    ]
    names_sent = send(ids.at[0], far_ids, rim_send.at[2], rim_recv.at[2], partner(near), part)
    gain_load.wait()
    scoped("norm_0", norm_tokens, 0)
    weight_loads = [
        load(source, held, weight_sem.at[i])
        for i, (source, held) in enumerate(
            (
                (out_hbm, out_weight),
                (shared_gate_hbm, shared_gate),
                (shared_up_hbm, shared_up),
                (shared_down_hbm, shared_down),
                (gate_hbm, gate),
                (up_hbm, up),
                (down_hbm, down),
            )
        )
    ]
    found_own = scoped("lay_out_0", lay_out, ids[0], rank)
    scoped("norm_1", norm_tokens, 1)
    found_peer = scoped("lay_out_1", lay_out, ids[1], rank)

    def give(n, source, which, count):
        dispatched[n] = send(
            source,
            rows.at[spot_of[n], pl.ds(which, count)],
            out_send.at[n],
            out_recv.at[n],
            partner(n if n < near else n - near),
            part,
        )

    for n in range(1, near):
        near_out[n - 1, 0:1] = scoped("near_rows", slot_rows, found_own, tok.at[0], n, 1)
        if n < direct:
            near_out[n - 1, 1:2] = scoped("near_rows", slot_rows, found_peer, tok.at[1], n, 1)
            give(n, near_out.at[n - 1], 0, 2)
        else:
            give(n, near_out.at[n - 1, pl.ds(0, 1)], 0, 1)
        if n == 1:
            dense_sent = send(
                tok.at[0], far_tok, out_send.at[0], out_recv.at[0], partner(near), part
            )
    rows[spot_of[0], 0:1] = scoped("rows", slot_rows, found_own, tok.at[0], 0, 1)
    rows[spot_of[0], 1:2] = scoped("rows", slot_rows, found_peer, tok.at[1], 0, 1)

    def proxy():
        arrive(names_sent)
        arrive(dense_sent)
        found = lay_out(far_ids[...], partner(near))
        s = spot_of[near]
        rows[s, 0:1] = slot_rows(found, far_tok, near, 1)
        fan(near)
        for n in (5, 6, 7):
            far_out[n - near - 1] = slot_rows(found, far_tok, n, 1)[0]
            give(n, far_out.at[pl.ds(n - near - 1, 1)], 0, 1)

    def layouts():
        keep_layout(0, found_own)
        keep_layout(1, found_peer)
        keep_route()

    low = lax.broadcasted_iota(i32, (BLOCK, 128), 1) < HEAD_DIM

    def head_scale(values, gain):
        squares = values * values
        lower = jnp.sum(jnp.where(low, squares, 0.0), axis=1, keepdims=True)
        upper = jnp.sum(jnp.where(low, 0.0, squares), axis=1, keepdims=True)
        mean = jnp.where(low, lower, upper) * (1.0 / HEAD_DIM)
        return values * lax.rsqrt(mean + epsilon) * gain

    def doubled(gain):
        return jnp.concatenate([gain[...], gain[...]], axis=1)

    def band_block(index, carry):
        at = pl.ds(pl.multiple_of(index * BLOCK, BLOCK), BLOCK)
        keys = head_scale(key_all[at].astype(f32), doubled(key_gain))
        values = value_all[at].astype(f32)
        for wide, band in ((keys, key_band), (values, value_band)):
            turned = pltpu.roll(wide, HEAD_DIM, 1)
            band[0, 0, at] = jnp.where(low, wide, 0.0).astype(bf16)
            band[0, 1, at] = jnp.where(low, 0.0, turned).astype(bf16)
            band[1, 0, at] = jnp.where(low, turned, 0.0).astype(bf16)
            band[1, 1, at] = jnp.where(low, 0.0, wide).astype(bf16)
        return carry

    def attend(n, slot):
        at = pl.ds(pl.multiple_of(n * BLOCK, BLOCK), BLOCK)
        span = pl.ds(pl.multiple_of(n * BLOCK, BLOCK), 2 * BLOCK)
        query_pos = lax.broadcasted_iota(i32, (BLOCK, 2 * BLOCK), 0)
        key_pos = lax.broadcasted_iota(i32, (BLOCK, 2 * BLOCK), 1)
        floor = jnp.where(rank * blocks + n > 0, 0, BLOCK)
        inside = (key_pos <= query_pos + BLOCK) & (key_pos > query_pos + BLOCK - WINDOW)
        inside = inside & (key_pos >= floor)
        for pair in range(pairs):
            kv = pair * 2 // (HEADS // KV_HEADS)
            lanes = slice(pair * 128, pair * 128 + 128)
            normed = head_scale(query[at, lanes].astype(f32), doubled(query_gain)).astype(bf16)
            keys = key_band[kv, :, span].reshape(4 * BLOCK, 128)
            scores = lax.dot_general(
                normed, keys, (((1,), (1,)), ((), ())), preferred_element_type=f32
            )
            probs = []
            for h in range(2):
                logit = sink[2 * pair + h]
                score = scores[:, h * 2 * BLOCK : (h + 1) * 2 * BLOCK] * score_scale
                score = jnp.where(inside, score, masked_score)
                top = jnp.maximum(jnp.max(score, axis=1, keepdims=True), logit)
                raised = jnp.exp(score - top)
                below = jnp.sum(raised, axis=1, keepdims=True) + jnp.exp(logit - top)
                probs.append((raised * (1.0 / below)).astype(bf16))
            values = value_band[kv, :, span].reshape(4 * BLOCK, 128)
            made = jnp.dot(jnp.concatenate(probs, axis=1), values, preferred_element_type=f32)
            heads[slot, :, lanes] = made.astype(bf16)

    def attention():
        query_load.wait()
        lax.fori_loop(1, blocks + 1, band_block, 0)
        for rim in rims:
            arrive(rim)
        band_block(0, 0)

        def one(j, carry):
            high = lax.rem(j, 2)
            turn = j // 2
            n = 2 * (side + high - 2 * side * high) + core + turn - 2 * core * turn
            attend(n, j)
            return carry

        lax.fori_loop(0, 4, one, 0)

    def early_pair(i, full, received):
        return send(
            full.at[pl.ds(2, 2)], received, early_send.at[i], early_recv.at[i], rank, sibling
        )

    early = {}
    flushes = []

    def mixer():
        weight_loads[0].wait()
        for half in (1, 0):
            held = heads[2 * half : 2 * half + 2].reshape(2 * quarter, heads.shape[-1])

            def one(c, carry):
                at = pl.ds(pl.multiple_of(c * chunk, chunk), chunk)
                made = jnp.dot(held, out_weight[:, at], preferred_element_type=f32)
                mixer_part[2 * half : 2 * half + 2, :, at] = made.astype(bf16).reshape(
                    2, quarter, chunk
                )
                return carry

            lax.fori_loop(0, chunks, one, 0)
            if half:
                early["mixer"] = early_pair(0, mixer_part, mixer_recv)

    def shared():
        for i in (1, 2, 3):
            weight_loads[i].wait()
        for half in (1, 0):
            held = tok[2 * half : 2 * half + 2].reshape(2 * quarter, width)
            gate_part = jnp.dot(held, shared_gate[...], preferred_element_type=f32)
            up_part = jnp.dot(held, shared_up[...], preferred_element_type=f32)
            hidden = (gate_part / (1.0 + jnp.exp(-gate_part)) * up_part).astype(bf16)

            def one(c, carry):
                at = pl.ds(pl.multiple_of(c * chunk, chunk), chunk)
                made = jnp.dot(hidden, shared_down[:, at], preferred_element_type=f32)
                shared_part[2 * half : 2 * half + 2, :, at] = made.astype(bf16).reshape(
                    2, quarter, chunk
                )
                return carry

            lax.fori_loop(0, chunks, one, 0)
            if half:
                early["shared"] = early_pair(1, shared_part, shared_recv)

    def mixer_add():
        arrive(early["mixer"])
        mixer_send[...] = (mixer_part[1].astype(f32) + mixer_recv[1].astype(f32)).astype(bf16)
        early["peer"] = send(
            mixer_send, mixer_peer, early_send.at[2], early_recv.at[2], rank, peer
        )

    def mixer_finish():
        arrive(early["peer"])
        results[0] = (
            mixer_part[0].astype(f32) + mixer_recv[0].astype(f32) + mixer_peer[...].astype(f32)
        ).astype(bf16)
        flushes.append(load(results.at[0], outputs.at[0], flush_sem.at[chunks]))

    def pass_on(k, sem, which, count):
        s = spot_of[k]
        return send(
            rows.at[s, pl.ds(which, count)],
            rows.at[s, pl.ds(2 + which, count)],
            fan_send.at[sem, k],
            fan_recv.at[sem, k],
            rank,
            sibling,
        )

    def fan(k):
        s = spot_of[k]
        if k not in (0, near):
            arrive(dispatched[k])
        if k >= direct:
            to_peer[k] = send(
                rows.at[s, 0], rows.at[s, 1], fan_send.at[0, k], fan_recv.at[0, k], rank, peer
            )
            to_sibling[k] = pass_on(k, 1, 0, 1)
        else:
            to_sibling[k] = pass_on(k, 1, 0, 2)

    def relay(k):
        arrive(to_peer[k])
        relayed[k] = pass_on(k, 2, 1, 1)

    ready = []

    def experts(*names):
        count = len(names)
        first = spot_of[names[0]]
        for k in names:
            arrive(to_sibling[k])
            if k in relayed:
                arrive(relayed[k])
        if not ready:
            for i in (4, 5, 6):
                weight_loads[i].wait()
            ready.append(True)

        def one(index, carry):
            at = pl.ds(pl.multiple_of(index * capacity, capacity), capacity)
            block = rows[first : first + count, :, at, :].reshape(count * 4 * capacity, width)
            gate_part = jnp.dot(block, gate[index], preferred_element_type=f32)
            up_part = jnp.dot(block, up[index], preferred_element_type=f32)
            hidden = (gate_part / (1.0 + jnp.exp(-gate_part)) * up_part).astype(bf16)
            made = jnp.dot(hidden, down[index], preferred_element_type=f32)
            made = made.astype(bf16).reshape(count, 4, capacity, width)
            spot = pl.ds(first, count)
            kept[spot, :, at, :] = made[:, 0:2]
            sibling_send[spot, :, at, :] = made[:, 2:4]
            return carry

        lax.fori_loop(0, local_experts, one, 0)
        for k in names:
            s = spot_of[k]
            added[k] = send(
                sibling_send.at[s],
                sibling_recv.at[s],
                add_send.at[0, k],
                add_recv.at[0, k],
                rank,
                sibling,
            )

    def add_pair(k):
        s = spot_of[k]
        arrive(added[k])
        if k >= near:
            kept[s, 1] = (kept[s, 1].astype(f32) + sibling_recv[s, 1].astype(f32)).astype(bf16)
            peered[k] = send(
                kept.at[s, 1],
                peer_recv.at[k - near],
                add_send.at[1, k],
                add_recv.at[1, k],
                rank,
                peer,
            )
            return
        both = (kept[s].astype(f32) + sibling_recv[s].astype(f32)).astype(bf16)
        if k == 0:
            near_back[0] = both
            return
        kept[s] = both

    def give_back(k):
        backs[k] = send(
            kept.at[spot_of[k]],
            near_back.at[k],
            back_send.at[k],
            back_recv.at[k],
            partner(k),
            part,
        )

    def finish(k):
        s = spot_of[k]
        arrive(peered[k])
        kept[s, 0] = (
            kept[s, 0].astype(f32)
            + sibling_recv[s, 0].astype(f32)
            + peer_recv[k - near].astype(f32)
        ).astype(bf16)
        backs[k] = send(
            kept.at[s, 0], far_back.at[k - near], back_send.at[k], back_recv.at[k], partner(k), part
        )

    def picked(j, source, first):
        count = source.shape[0]
        slots = lax.broadcasted_iota(i32, (quarter, count), 1) + first
        result = 0
        for i in range(TOP_K):
            hot = (spots[j, :, i : i + 1] == slots).astype(bf16)
            result = result + jnp.dot(hot, source, preferred_element_type=f32) * picks[
                j, :, i : i + 1
            ]
        return result

    def near_sum(j):
        if j:
            for k in range(1, near):
                arrive(backs[k])
            arrive(early["shared"])

        def one(c, carry):
            at = pl.ds(pl.multiple_of(c * chunk, chunk), chunk)
            source = near_back[:, j, :, at].reshape(near * share, chunk)
            value = (
                shared_part[j, :, at].astype(f32)
                + shared_recv[j, :, at].astype(f32)
                + picked(j, source, 0)
            )
            if j:
                merged_send[:, at] = value.astype(bf16)
            else:
                total[:, at] = value
            return carry

        lax.fori_loop(0, chunks, one, 0)
        if j:
            early["merged"] = send(
                merged_send, merged_recv, early_send.at[3], early_recv.at[3], rank, peer
            )

    def far_sum(first, count):
        last = first + count == ranks
        for k in range(first, first + count):
            arrive(backs[k])
        if last:
            arrive(early["merged"])

        def one(c, carry):
            at = pl.ds(pl.multiple_of(c * chunk, chunk), chunk)
            source = far_back[first - near : first - near + count, :, at].reshape(
                count * share, chunk
            )
            value = total[:, at] + picked(0, source, first * share)
            if last:
                value = value + merged_recv[:, at].astype(f32)
                results[1, :, at] = value.astype(bf16)
            else:
                total[:, at] = value
            return carry

        if last:
            for c in range(chunks):
                one(c, 0)
                at = pl.ds(c * chunk, chunk)
                flushes.append(
                    load(results.at[1, :, at], outputs.at[1, :, at], flush_sem.at[c])
                )
        else:
            lax.fori_loop(0, chunks, one, 0)

    steps = {
        "proxy": proxy,
        "layouts": layouts,
        "norm": norm_tokens,
        "attention": attention,
        "mixer": mixer,
        "shared": shared,
        "mixer_add": mixer_add,
        "mixer_finish": mixer_finish,
        "fan": fan,
        "relay": relay,
        "experts": experts,
        "add": add_pair,
        "back": give_back,
        "finish": finish,
        "near_sum": near_sum,
        "far_sum": far_sum,
    }
    for name, *settings in program:
        with jax.named_scope("_".join(map(str, (name, *settings)))):
            steps[name](*settings)
    for copy in sent:
        copy.wait_send()
    for copy in flushes:
        copy.wait()


def step_order(direct):
    program = (
        ("fan", 0), ("attention",), ("fan", 1), ("fan", 2), ("fan", 3), ("proxy",),
        ("experts", 0, 1), ("relay", 2), ("add", 0), ("relay", 3), ("fan", 5),
        ("experts", 2, 3), ("relay", 4), ("fan", 6), ("add", 3), ("back", 3), ("relay", 5),
        ("add", 2), ("fan", 7), ("experts", 4), ("experts", 5), ("norm", 2), ("add", 1),
        ("mixer",), ("add", 5), ("norm", 3), ("back", 2), ("back", 1), ("add", 4), ("shared",),
        ("relay", 6), ("finish", 5), ("layouts",), ("mixer_add",), ("relay", 7), ("finish", 4),
        ("experts", 6, 7), ("add", 6), ("add", 7), ("near_sum", 1), ("mixer_finish",),
        ("finish", 6), ("near_sum", 0), ("finish", 7), ("far_sum", 6, 1), ("far_sum", 4, 2),
        ("far_sum", 7, 1),
    )
    return [step for step in program if step[0] != "relay" or step[1] >= direct]


def layer(arrays, local_experts, capacity, ranks):
    query_rows, out_weight, tokens, gate, up, down, shared_gate, shared_up, shared_down = arrays[1]
    near, direct = 4, 2
    order = tuple(range(ranks))
    bf16, f32 = jnp.bfloat16, jnp.float32
    dma = pltpu.SemaphoreType.DMA
    quarter = tokens.shape[0] // 4
    width = tokens.shape[1]
    share = local_experts * capacity
    sequence = query_rows.shape[0]
    far = ranks - near
    vmem = pl.BlockSpec(memory_space=pltpu.VMEM)
    anywhere = pl.BlockSpec(memory_space=pl.ANY)
    smem = pl.BlockSpec(memory_space=pltpu.SMEM)

    def held(*shape):
        return pltpu.VMEM(shape, bf16)

    return pl.pallas_call(
        functools.partial(
            layer_kernel, ranks, near, direct, order, step_order(direct), local_experts, capacity
        ),
        out_shape=jax.ShapeDtypeStruct((2, quarter, width), bf16),
        in_specs=[smem]
        + [anywhere] * 3
        + [vmem] * 2
        + [anywhere] * 11,
        out_specs=anywhere,
        scratch_shapes=[
            held(2, quarter, width),
            dma((width // 512 + 1,)),
            held(ranks, 4, share, width),
            held(ranks, 2, share, width),
            held(ranks, 2, share, width),
            held(ranks, 2, share, width),
            held(far, share, width),
            held(far - 1, share, width),
            held(near - 1, 2, share, width),
            held(far, share, width),
            held(near, 2, share, width),
            held(4, quarter, width),
            held(4, quarter, width),
            held(2, quarter, width),
            held(2, quarter, width),
            held(quarter, width),
            held(quarter, width),
            held(quarter, width),
            held(quarter, width),
            pltpu.VMEM((quarter, width), f32),
            held(4, quarter, width),
            held(*query_rows.shape),
            held(sequence + BLOCK, 128),
            held(sequence + BLOCK, 128),
            held(2, 2, sequence + BLOCK, 128),
            held(2, 2, sequence + BLOCK, 128),
            held(4, quarter, query_rows.shape[1]),
            pltpu.VMEM((2, TOP_K, quarter), jnp.int32),
            pltpu.VMEM((2, TOP_K, quarter), f32),
            pltpu.VMEM((2, quarter, TOP_K), jnp.int32),
            pltpu.VMEM((2, quarter, TOP_K), f32),
            pltpu.VMEM((1, width), f32),
            held(quarter, width),
            pltpu.VMEM((TOP_K, quarter), jnp.int32),
            held(*gate.shape),
            held(*up.shape),
            held(*down.shape),
            held(*out_weight.shape),
            held(*shared_gate.shape),
            held(*shared_up.shape),
            held(*shared_down.shape),
            dma((4,)),
            dma((8,)),
            dma((7,)),
            dma((3,)),
            dma((3,)),
            dma((ranks,)),
            dma((ranks,)),
            dma((3, ranks)),
            dma((3, ranks)),
            dma((2, ranks)),
            dma((2, ranks)),
            dma((ranks,)),
            dma((ranks,)),
            dma((4,)),
            dma((4,)),
        ],
        compiler_params=pltpu.CompilerParams(
            collective_id=0, has_side_effects=True, vmem_limit_bytes=65000 * 1024
        ),
    )(*arrays[0])


def wide_shards(
    query_rows,
    key_rows,
    value_rows,
    query_gain,
    key_gain,
    sink_logit,
    out_weight,
    tokens,
    norm_gain,
    expert_ids,
    route_weight,
    gate_weight,
    up_weight,
    down_weight,
    shared_gate,
    shared_up,
    shared_down,
):
    expert_ranks = lax.axis_size("ep")
    head_ranks = lax.axis_size("tp")
    head_rank = lax.axis_index("tp")
    sequence_rows = query_rows.shape[0]
    blocks = sequence_rows // BLOCK
    pair_heads = key_rows.shape[1] // HEAD_DIM
    group_size = HEADS // KV_HEADS
    query_normed = rms_scale(
        query_rows.reshape(blocks, BLOCK, pair_heads, group_size, HEAD_DIM), query_gain
    )
    key_normed = rms_scale(key_rows.reshape(blocks, BLOCK, pair_heads, HEAD_DIM), key_gain)
    value_blocks = value_rows.reshape(blocks, BLOCK, pair_heads, HEAD_DIM)
    rim_keys, rim_values = from_behind((key_normed[blocks - 1], value_blocks[blocks - 1]), "ep", 1)
    key_band = band_blocks(rim_keys, key_normed)
    value_band = band_blocks(rim_values, value_blocks)
    window = window_mask(lax.axis_index("ep") * blocks, blocks)
    scores = (
        jnp.einsum("nqhgd,nkhd->hgnqk", query_normed, key_band, preferred_element_type=jnp.float32)
        * score_scale
    )
    scores = jnp.where(window[None, None], scores, masked_score)
    sink_col = sink_logit.reshape(pair_heads, group_size, 1, 1, 1)
    row_max = jnp.maximum(jnp.max(scores, axis=-1, keepdims=True), sink_col)
    exp_scores = jnp.exp(scores - row_max)
    attn_probs = (
        exp_scores / (jnp.sum(exp_scores, axis=-1, keepdims=True) + jnp.exp(sink_col - row_max))
    ).astype(jnp.bfloat16)
    heads_out = (
        jnp.einsum("hgnqk,nkhd->nqhgd", attn_probs, value_band, preferred_element_type=jnp.float32)
        .astype(jnp.bfloat16)
        .reshape(sequence_rows, pair_heads * group_size * HEAD_DIM)
    )
    local_experts = gate_weight.shape[0]
    expert_total = local_experts * expert_ranks
    quarter = tokens.shape[0] // head_ranks
    model_width = tokens.shape[1]
    capacity = 2 * quarter * TOP_K // expert_total
    slot_share = local_experts * capacity
    routed_rows = expert_ranks * slot_share
    normed = rms_scale(tokens, norm_gain)
    route_ids = expert_ids.reshape(head_ranks, quarter * TOP_K)
    one_hot = (route_ids[:, :, None] == jnp.arange(expert_total, dtype=jnp.int32)).astype(jnp.int32)
    slot_rank = jnp.sum(one_hot * (jnp.cumsum(one_hot, axis=1) - 1), axis=-1)
    positions = route_ids * capacity + slot_rank
    owners = jnp.arange(quarter * TOP_K, dtype=jnp.int32) // TOP_K
    padded_rows = jnp.concatenate(
        [
            normed.reshape(head_ranks, quarter, model_width),
            jnp.zeros((head_ranks, 1, model_width), jnp.bfloat16),
        ],
        axis=1,
    ).reshape(head_ranks * (quarter + 1), model_width)
    slot_token = (
        jnp.full((head_ranks, routed_rows), quarter, jnp.int32)
        .at[jnp.arange(head_ranks, dtype=jnp.int32)[:, None], positions]
        .set(jnp.broadcast_to(owners[None, :], positions.shape))
    )
    slot_index = slot_token + (jnp.arange(head_ranks, dtype=jnp.int32) * (quarter + 1))[:, None]
    own_index = lax.dynamic_index_in_dim(slot_index, head_rank, 0, keepdims=True)
    outgoing = padded_rows[own_index].reshape(1, expert_ranks, slot_share, model_width)
    arrived = lax.all_to_all(outgoing, "ep", split_axis=1, concat_axis=1, tiled=True)
    piece_rows = lax.all_gather(
        arrived.reshape(1, expert_ranks, local_experts, capacity, model_width),
        "tp",
        axis=0,
        tiled=True,
    )
    gate_part = jnp.einsum(
        "tsecd,edf->tsecf", piece_rows, gate_weight, preferred_element_type=jnp.float32
    )
    up_part = jnp.einsum(
        "tsecd,edf->tsecf", piece_rows, up_weight, preferred_element_type=jnp.float32
    )
    hidden = (jax.nn.silu(gate_part) * up_part).astype(jnp.bfloat16)
    shared_hidden = (
        jax.nn.silu(jnp.dot(normed, shared_gate, preferred_element_type=jnp.float32))
        * jnp.dot(normed, shared_up, preferred_element_type=jnp.float32)
    ).astype(jnp.bfloat16)
    span_rows = routed_rows + quarter
    mixer_out = lax.psum_scatter(
        jnp.dot(heads_out, out_weight, preferred_element_type=jnp.float32).astype(jnp.bfloat16),
        "tp",
        scatter_dimension=0,
        tiled=True,
    )
    part_count = lax.axis_size("tp") * span_rows // span_rows
    routed_part = jnp.einsum(
        "tsecf,efd->tsecd", hidden, down_weight, preferred_element_type=jnp.float32
    ).reshape(part_count, routed_rows, model_width)
    shared_part = jnp.dot(shared_hidden, shared_down, preferred_element_type=jnp.float32).reshape(
        part_count, quarter, model_width
    )
    summed = lax.psum_scatter(
        jnp.concatenate([routed_part, shared_part], axis=1)
        .reshape(part_count * span_rows, model_width)
        .astype(jnp.bfloat16),
        "tp",
        scatter_dimension=0,
        tiled=True,
    )
    returned = lax.all_to_all(
        summed[:routed_rows].reshape(expert_ranks, slot_share, model_width),
        "ep",
        split_axis=0,
        concat_axis=0,
        tiled=True,
    ).reshape(routed_rows, model_width)
    own_positions = lax.dynamic_index_in_dim(positions, head_rank, 0, keepdims=False)
    picked = returned[own_positions].reshape(quarter, TOP_K, model_width).astype(jnp.float32)
    own_weights = lax.dynamic_slice_in_dim(route_weight, head_rank * quarter, quarter, 0)
    expert_out = (
        summed[routed_rows:].astype(jnp.float32) + jnp.sum(picked * own_weights[:, :, None], axis=1)
    ).astype(jnp.bfloat16)
    return (mixer_out, expert_out)


def shards(
    query_rows,
    key_rows,
    value_rows,
    query_gain,
    key_gain,
    sink_logit,
    out_weight,
    tokens,
    norm_gain,
    expert_ids,
    route_weight,
    gate_weight,
    up_weight,
    down_weight,
    shared_gate,
    shared_up,
    shared_down,
):
    expert_ranks = lax.axis_size("ep")
    head_ranks = lax.axis_size("tp")
    local_experts = gate_weight.shape[0]
    expert_total = local_experts * expert_ranks
    quarter = tokens.shape[0] // head_ranks
    capacity = 2 * quarter * TOP_K // expert_total
    fits = (
        head_ranks == 4
        and expert_ranks == 8
        and capacity % 16 == 0
        and quarter == BLOCK
        and query_rows.shape[0] == 4 * BLOCK
        and key_rows.shape[1] == 2 * HEAD_DIM
    )
    if not fits:
        return wide_shards(
            query_rows,
            key_rows,
            value_rows,
            query_gain,
            key_gain,
            sink_logit,
            out_weight,
            tokens,
            norm_gain,
            expert_ids,
            route_weight,
            gate_weight,
            up_weight,
            down_weight,
            shared_gate,
            shared_up,
            shared_down,
        )
    operands = (
        sink_logit,
        query_rows,
        key_rows,
        value_rows,
        query_gain.reshape(1, HEAD_DIM),
        key_gain.reshape(1, HEAD_DIM),
        out_weight,
        tokens,
        norm_gain.reshape(1, tokens.shape[1]),
        expert_ids.T,
        route_weight.T,
        gate_weight,
        up_weight,
        down_weight,
        shared_gate,
        shared_up,
        shared_down,
    )
    shaped = (
        query_rows,
        out_weight,
        tokens,
        gate_weight,
        up_weight,
        down_weight,
        shared_gate,
        shared_up,
        shared_down,
    )
    both = layer((operands, shaped), local_experts, capacity, expert_ranks)
    return both[0], both[1]


def solution(mesh):
    in_specs = (
        P("ep", "tp"),
        P("ep", "tp"),
        P("ep", "tp"),
        P(),
        P(),
        P("tp"),
        P("tp", None),
        P("ep", None),
        P(),
        P("ep", None),
        P("ep", None),
        P("ep", None, "tp"),
        P("ep", None, "tp"),
        P("ep", "tp", None),
        P(None, "tp"),
        P(None, "tp"),
        P("tp", None),
    )
    out_specs = (P(("ep", "tp"), None), P(("ep", "tp"), None))
    return jax.shard_map(shards, mesh=mesh, in_specs=in_specs, out_specs=out_specs, check_vma=False)
```

```python
import functools
import jax
import jax.numpy as jnp
from jax import lax
from jax.experimental import pallas as pl
from jax.experimental.pallas import tpu as pltpu
from jax.sharding import PartitionSpec as P

HEADS = 32
KV_HEADS = 8
HEAD_DIM = 64
WINDOW = 128
BLOCK = 128
TOP_K = 2


epsilon = 1e-06
masked_score = -1e30
score_scale = 0.125


def from_behind(block, axis, distance):
    devices = range(lax.axis_size(axis))
    route = [(i - distance, i) for i in devices if i - distance in devices]
    return lax.ppermute(block, axis, route)


def rms_scale(values, gain):
    widened = values.astype(jnp.float32)
    scaled = widened * lax.rsqrt(jnp.mean(widened * widened, axis=-1, keepdims=True) + epsilon)
    return (scaled * gain).astype(jnp.bfloat16)


def window_mask(first_block, block_count):
    query_pos = jnp.arange(BLOCK)[:, None]
    key_pos = jnp.arange(2 * BLOCK)[None, :]
    inside = (key_pos <= query_pos + BLOCK) & (key_pos > query_pos + BLOCK - WINDOW)
    not_first = (first_block + jnp.arange(block_count))[:, None, None] > 0
    return inside[None] & (not_first | (key_pos[None] >= BLOCK))


def band_blocks(rim_block, blocks_in):
    joined = jnp.concatenate([rim_block[None], blocks_in], axis=0)
    return jnp.concatenate([joined[:-1], joined[1:]], axis=1)


def layer_kernel(
    ranks,
    near,
    direct,
    order,
    program,
    local_experts,
    capacity,
    sink,
    query_hbm,
    key_hbm,
    value_hbm,
    query_gain_hbm,
    key_gain_hbm,
    out_hbm,
    tokens_hbm,
    gain_hbm,
    ids_hbm,
    route_hbm,
    gate_hbm,
    up_hbm,
    down_hbm,
    shared_gate_hbm,
    shared_up_hbm,
    shared_down_hbm,
    outputs,
    results,
    flush_sem,
    query_gain,
    key_gain,
    head_sem,
    rows,
    kept,
    sibling_send,
    sibling_recv,
    peer_recv,
    far_out,
    near_out,
    far_back,
    near_back,
    mixer_part,
    shared_part,
    mixer_recv,
    shared_recv,
    mixer_send,
    mixer_peer,
    merged_send,
    merged_recv,
    total,
    tok,
    query,
    key_all,
    value_all,
    key_band,
    value_band,
    heads,
    ids,
    route,
    spots,
    picks,
    norm_gain,
    far_tok,
    far_ids,
    gate,
    up,
    down,
    out_weight,
    shared_gate,
    shared_up,
    shared_down,
    tok_sem,
    small_sem,
    weight_sem,
    rim_send,
    rim_recv,
    out_send,
    out_recv,
    fan_send,
    fan_recv,
    add_send,
    add_recv,
    back_send,
    back_recv,
    early_send,
    early_recv,
):
    rank = lax.axis_index("ep")
    part = lax.axis_index("tp")
    core = lax.rem(part, 2)
    side = part // 2
    sibling = 2 * side + 1 - core
    peer = 2 * (1 - side) + core
    across = 2 * (1 - side) + 1 - core
    placed = (part, peer, sibling, across)
    f32, bf16, i32 = jnp.float32, jnp.bfloat16, jnp.int32
    mesh_ids = pl.DeviceIdType.MESH
    width = rows.shape[-1]
    quarter = tok.shape[1]
    share = rows.shape[2]
    blocks = query.shape[0] // BLOCK
    pairs = query.shape[1] // 128
    spot_of = {k: s for s, k in enumerate(order)}
    chunk = 512
    chunks = width // chunk

    def partner(k):
        result = 0
        bit = 1
        while bit < ranks:
            own = lax.rem(rank // bit, 2)
            result = result + bit * ((1 - own) if k & bit else own)
            bit *= 2
        return result

    def send(source, target, send_sem, recv_sem, ep_to, tp_to):
        copy = pltpu.make_async_remote_copy(
            src_ref=source,
            dst_ref=target,
            send_sem=send_sem,
            recv_sem=recv_sem,
            device_id=(ep_to, tp_to),
            device_id_type=mesh_ids,
        )
        copy.start()
        sent.append(copy)
        return copy

    def arrive(copy):
        with jax.named_scope("wait"):
            copy.wait_recv()

    sent = []
    barrier = pltpu.get_barrier_semaphore()
    ahead = lax.rem(rank + 1, ranks)
    behind = lax.rem(rank + ranks - 1, ranks)
    for k in range(1, ranks):
        pl.semaphore_signal(barrier, inc=1, device_id=(partner(k), part), device_id_type=mesh_ids)
    for other in (sibling, peer):
        pl.semaphore_signal(barrier, inc=1, device_id=(rank, other), device_id_type=mesh_ids)

    def load(source, target, sem):
        copy = pltpu.make_async_copy(source, target, sem)
        copy.start()
        return copy

    def block_at(j):
        return pl.ds(pl.multiple_of(placed[j] * quarter, quarter), quarter)

    tok_loads = [load(tokens_hbm.at[block_at(j)], tok.at[j], tok_sem.at[j]) for j in range(4)]
    head_loads = [
        load(source, held, head_sem.at[i])
        for i, (source, held) in enumerate(
            ((query_gain_hbm, query_gain), (key_gain_hbm, key_gain))
        )
    ]
    gain_load = load(gain_hbm, norm_gain, small_sem.at[0])
    id_loads = [load(ids_hbm.at[:, block_at(j)], ids.at[j], small_sem.at[1 + j]) for j in range(2)]
    sequence = query.shape[0]
    query_load = load(query_hbm, query, small_sem.at[5])
    key_load = load(key_hbm, key_all.at[pl.ds(BLOCK, sequence)], small_sem.at[6])
    value_load = load(value_hbm, value_all.at[pl.ds(BLOCK, sequence)], small_sem.at[7])
    route_loads = [
        load(route_hbm.at[:, block_at(j)], route.at[j], small_sem.at[3 + j]) for j in range(2)
    ]

    def norm_tokens(j):
        scoped("load", tok_loads[j].wait)
        wide = tok[j].astype(f32)
        scaled = wide * lax.rsqrt(jnp.mean(wide * wide, axis=-1, keepdims=True) + epsilon)
        tok[j] = (scaled * norm_gain[...]).astype(bf16)

    def bits(value, other):
        result = 0
        bit = 1
        while bit < ranks:
            own = lax.rem(other // bit, 2)
            theirs = lax.rem(value // bit, 2)
            result = result + bit * (theirs + own - 2 * theirs * own)
            bit *= 2
        return result

    def lay_out(named, source):
        experts_all = local_experts * ranks
        labels = lax.broadcasted_iota(i32, (experts_all, quarter), 0)
        behind_of = lax.broadcasted_iota(i32, (quarter, quarter), 0)
        below = (behind_of < lax.broadcasted_iota(i32, (quarter, quarter), 1)).astype(bf16)
        lines = [named[i : i + 1, :] for i in range(TOP_K)]
        hot = [(line == labels).astype(f32) for line in lines]
        before = jnp.dot(sum(hot).astype(bf16), below, preferred_element_type=f32)
        found = []
        for i, line in enumerate(lines):
            within = jnp.sum(hot[i] * before, axis=0, keepdims=True).astype(i32)
            ahead_of = bits(line // local_experts, source)
            found.append(ahead_of * share + lax.rem(line, local_experts) * capacity + within)
        return found

    def upright(line):
        return jnp.transpose(jnp.broadcast_to(line, (quarter, quarter)))[:, 0:1]

    def keep_layout(j, found):
        for i in range(TOP_K):
            spots[j, :, i : i + 1] = upright(found[i].astype(f32)).astype(i32)

    def keep_route():
        for j in range(2):
            route_loads[j].wait()
            for i in range(TOP_K):
                picks[j, :, i : i + 1] = upright(route[j, i : i + 1, :])

    def slot_rows(found, source, k, count):
        used = lax.broadcasted_iota(i32, (count * share, quarter), 0) + k * share
        chosen = sum((used == spot).astype(bf16) for spot in found)
        made = jnp.dot(chosen, source[...], preferred_element_type=f32)
        return made.astype(bf16).reshape(count, share, made.shape[1])

    dispatched = {}
    to_sibling = {}
    to_peer = {}
    relayed = {}
    added = {}
    peered = {}
    backs = {}

    def scoped(name, work, *settings):
        with jax.named_scope(name):
            return work(*settings)

    scoped("barrier", pl.semaphore_wait, barrier, ranks + 1)
    for copy in (key_load, value_load, *id_loads):
        copy.wait()
    rims = [
        send(
            held.at[pl.ds(sequence, BLOCK)],
            held.at[pl.ds(0, BLOCK)],
            rim_send.at[i],
            rim_recv.at[i],
            ahead,
            part,
        )
        for i, held in enumerate((key_all, value_all))
    ]
    names_sent = send(ids.at[0], far_ids, rim_send.at[2], rim_recv.at[2], partner(near), part)
    gain_load.wait()
    scoped("norm_0", norm_tokens, 0)
    weight_loads = [
        load(source, held, weight_sem.at[i])
        for i, (source, held) in enumerate(
            (
                (out_hbm, out_weight),
                (shared_gate_hbm, shared_gate),
                (shared_up_hbm, shared_up),
                (shared_down_hbm, shared_down),
                (gate_hbm, gate),
                (up_hbm, up),
                (down_hbm, down),
            )
        )
    ]
    found_own = scoped("lay_out_0", lay_out, ids[0], rank)
    scoped("norm_1", norm_tokens, 1)
    found_peer = scoped("lay_out_1", lay_out, ids[1], rank)

    def give(n, source, target, h):
        return send(
            source,
            target,
            out_send.at[h, n],
            out_recv.at[h, n],
            partner(n if n < near else n - near),
            part,
        )

    halves = [pl.ds(h * (width // 2), width // 2) for h in range(2)]
    for n in range(1, near):
        near_out[n - 1, 0:1] = scoped("near_rows", slot_rows, found_own, tok.at[0], n, 1)
        if n < direct:
            near_out[n - 1, 1:2] = scoped("near_rows", slot_rows, found_peer, tok.at[1], n, 1)
            dispatched[n] = [give(n, near_out.at[n - 1], rows.at[spot_of[n], pl.ds(0, 2)], 0)]
        else:
            dispatched[n] = [give(n, near_out.at[n - 1, 0], rows.at[spot_of[n], 0], 0)]
        if n == 1:
            dense_sent = [
                send(
                    tok.at[0, :, columns],
                    far_tok.at[:, columns],
                    out_send.at[h, near],
                    out_recv.at[h, near],
                    partner(near),
                    part,
                )
                for h, columns in enumerate(halves)
            ]
    rows[spot_of[0], 0:1] = scoped("rows", slot_rows, found_own, tok.at[0], 0, 1)
    rows[spot_of[0], 1:2] = scoped("rows", slot_rows, found_peer, tok.at[1], 0, 1)

    def proxy(h):
        columns = halves[h]
        if h == 0:
            arrive(names_sent)
        arrive(dense_sent[h])
        found = lay_out(far_ids[...], partner(near))
        s = spot_of[near]
        source = far_tok.at[:, columns]
        rows[s, 0:1, :, columns] = slot_rows(found, source, near, 1)
        own = rows.at[s, 0, :, columns]
        to_peer.setdefault(near, []).append(
            send(
                own,
                rows.at[s, 1, :, columns],
                fan_send.at[3 * h, near],
                fan_recv.at[3 * h, near],
                rank,
                peer,
            )
        )
        to_sibling.setdefault(near, []).append(
            send(
                own,
                rows.at[s, 2, :, columns],
                fan_send.at[1 + 3 * h, near],
                fan_recv.at[1 + 3 * h, near],
                rank,
                sibling,
            )
        )
        for n in range(near + 1, ranks):
            far_out[n - near - 1, :, columns] = slot_rows(found, source, n, 1)[0]
            dispatched.setdefault(n, []).append(
                give(
                    n,
                    far_out.at[n - near - 1, :, columns],
                    rows.at[spot_of[n], 0, :, columns],
                    h,
                )
            )

    def layouts():
        keep_layout(0, found_own)
        keep_layout(1, found_peer)
        keep_route()

    low = lax.broadcasted_iota(i32, (BLOCK, 128), 1) < HEAD_DIM

    def head_scale(values, gain):
        squares = values * values
        lower = jnp.sum(jnp.where(low, squares, 0.0), axis=1, keepdims=True)
        upper = jnp.sum(jnp.where(low, 0.0, squares), axis=1, keepdims=True)
        mean = jnp.where(low, lower, upper) * (1.0 / HEAD_DIM)
        return values * lax.rsqrt(mean + epsilon) * gain

    def doubled(gain):
        return jnp.concatenate([gain[...], gain[...]], axis=1)

    def band_block(index, carry):
        at = pl.ds(pl.multiple_of(index * BLOCK, BLOCK), BLOCK)
        keys = head_scale(key_all[at].astype(f32), doubled(key_gain))
        values = value_all[at].astype(f32)
        for wide, band in ((keys, key_band), (values, value_band)):
            turned = pltpu.roll(wide, HEAD_DIM, 1)
            band[0, 0, at] = jnp.where(low, wide, 0.0).astype(bf16)
            band[0, 1, at] = jnp.where(low, 0.0, turned).astype(bf16)
            band[1, 0, at] = jnp.where(low, turned, 0.0).astype(bf16)
            band[1, 1, at] = jnp.where(low, 0.0, wide).astype(bf16)
        return carry

    def attend(n, slot):
        at = pl.ds(pl.multiple_of(n * BLOCK, BLOCK), BLOCK)
        span = pl.ds(pl.multiple_of(n * BLOCK, BLOCK), 2 * BLOCK)
        query_pos = lax.broadcasted_iota(i32, (BLOCK, 2 * BLOCK), 0)
        key_pos = lax.broadcasted_iota(i32, (BLOCK, 2 * BLOCK), 1)
        floor = jnp.where(rank * blocks + n > 0, 0, BLOCK)
        inside = (key_pos <= query_pos + BLOCK) & (key_pos > query_pos + BLOCK - WINDOW)
        inside = inside & (key_pos >= floor)
        for pair in range(pairs):
            kv = pair * 2 // (HEADS // KV_HEADS)
            lanes = slice(pair * 128, pair * 128 + 128)
            normed = head_scale(query[at, lanes].astype(f32), doubled(query_gain)).astype(bf16)
            keys = key_band[kv, :, span].reshape(4 * BLOCK, 128)
            scores = lax.dot_general(
                normed, keys, (((1,), (1,)), ((), ())), preferred_element_type=f32
            )
            probs = []
            for h in range(2):
                logit = sink[2 * pair + h]
                score = scores[:, h * 2 * BLOCK : (h + 1) * 2 * BLOCK] * score_scale
                score = jnp.where(inside, score, masked_score)
                top = jnp.maximum(jnp.max(score, axis=1, keepdims=True), logit)
                raised = jnp.exp(score - top)
                below = jnp.sum(raised, axis=1, keepdims=True) + jnp.exp(logit - top)
                probs.append((raised * (1.0 / below)).astype(bf16))
            values = value_band[kv, :, span].reshape(4 * BLOCK, 128)
            made = jnp.dot(jnp.concatenate(probs, axis=1), values, preferred_element_type=f32)
            heads[slot, :, lanes] = made.astype(bf16)

    def keys():
        for copy in (query_load, *head_loads):
            copy.wait()
        lax.fori_loop(1, blocks + 1, band_block, 0)
        for rim in rims:
            arrive(rim)
        band_block(0, 0)

    def attend_half(half):
        def one(step, carry):
            j = 2 * step + half
            n = 2 * (side + half - 2 * side * half) + core + step - 2 * core * step
            attend(n, j)
            return carry

        lax.fori_loop(0, 2, one, 0)

    def early_pair(i, full, received):
        return send(
            full.at[pl.ds(2, 2)], received, early_send.at[i], early_recv.at[i], rank, sibling
        )

    early = {}
    flushes = []

    def mixer(half):
        if half:
            weight_loads[0].wait()
        held = jnp.concatenate([heads[half], heads[2 + half]], axis=0)

        def one(c, carry):
            at = pl.ds(pl.multiple_of(c * chunk, chunk), chunk)
            made = jnp.dot(held, out_weight[:, at], preferred_element_type=f32).astype(bf16)
            mixer_part[half, :, at] = made[:quarter]
            mixer_part[2 + half, :, at] = made[quarter:]
            return carry

        lax.fori_loop(0, chunks, one, 0)
        early["mixer", half] = send(
            mixer_part.at[2 + half],
            mixer_recv.at[half],
            early_send.at[4 * half],
            early_recv.at[4 * half],
            rank,
            sibling,
        )

    def shared():
        for i in (1, 2, 3):
            weight_loads[i].wait()
        for half in (1, 0):
            held = tok[2 * half : 2 * half + 2].reshape(2 * quarter, width)
            gate_part = jnp.dot(held, shared_gate[...], preferred_element_type=f32)
            up_part = jnp.dot(held, shared_up[...], preferred_element_type=f32)
            hidden = (gate_part / (1.0 + jnp.exp(-gate_part)) * up_part).astype(bf16)

            def one(c, carry):
                at = pl.ds(pl.multiple_of(c * chunk, chunk), chunk)
                made = jnp.dot(hidden, shared_down[:, at], preferred_element_type=f32)
                shared_part[2 * half : 2 * half + 2, :, at] = made.astype(bf16).reshape(
                    2, quarter, chunk
                )
                return carry

            lax.fori_loop(0, chunks, one, 0)
            if half:
                early["shared"] = early_pair(1, shared_part, shared_recv)

    def mixer_add():
        arrive(early["mixer", 1])
        mixer_send[...] = (mixer_part[1].astype(f32) + mixer_recv[1].astype(f32)).astype(bf16)
        early["peer"] = send(
            mixer_send, mixer_peer, early_send.at[2], early_recv.at[2], rank, peer
        )

    def mixer_finish():
        arrive(early["mixer", 0])
        arrive(early["peer"])
        results[0] = (
            mixer_part[0].astype(f32) + mixer_recv[0].astype(f32) + mixer_peer[...].astype(f32)
        ).astype(bf16)
        flushes.append(load(results.at[0], outputs.at[0], flush_sem.at[chunks]))

    def pass_on(k, sem, which, count):
        s = spot_of[k]
        return send(
            rows.at[s, pl.ds(which, count)],
            rows.at[s, pl.ds(2 + which, count)],
            fan_send.at[sem, k],
            fan_recv.at[sem, k],
            rank,
            sibling,
        )

    def fan(k):
        s = spot_of[k]
        for copy in dispatched.get(k, ()):
            arrive(copy)
        if k >= direct:
            to_peer[k] = [
                send(
                    rows.at[s, 0], rows.at[s, 1], fan_send.at[0, k], fan_recv.at[0, k], rank, peer
                )
            ]
            to_sibling[k] = [pass_on(k, 1, 0, 1)]
        else:
            to_sibling[k] = [pass_on(k, 1, 0, 2)]

    def relay(k):
        for copy in to_peer[k]:
            arrive(copy)
        relayed[k] = pass_on(k, 2, 1, 1)

    ready = []

    def experts(*names):
        count = len(names)
        first = spot_of[names[0]]
        for k in names:
            for copy in to_sibling[k]:
                arrive(copy)
            if k in relayed:
                arrive(relayed[k])
        if not ready:
            for i in (4, 5, 6):
                weight_loads[i].wait()
            ready.append(True)

        def one(index, carry):
            at = pl.ds(pl.multiple_of(index * capacity, capacity), capacity)
            block = rows[first : first + count, :, at, :].reshape(count * 4 * capacity, width)
            gate_part = jnp.dot(block, gate[index], preferred_element_type=f32)
            up_part = jnp.dot(block, up[index], preferred_element_type=f32)
            hidden = (gate_part / (1.0 + jnp.exp(-gate_part)) * up_part).astype(bf16)
            made = jnp.dot(hidden, down[index], preferred_element_type=f32)
            made = made.astype(bf16).reshape(count, 4, capacity, width)
            spot = pl.ds(first, count)
            kept[spot, :, at, :] = made[:, 0:2]
            sibling_send[spot, :, at, :] = made[:, 2:4]
            return carry

        lax.fori_loop(0, local_experts, one, 0)
        for k in names:
            s = spot_of[k]
            added[k] = send(
                sibling_send.at[s],
                sibling_recv.at[s],
                add_send.at[0, k],
                add_recv.at[0, k],
                rank,
                sibling,
            )

    def add_pair(k):
        s = spot_of[k]
        arrive(added[k])
        if k >= near:
            for h, columns in enumerate(halves):
                kept[s, 1, :, columns] = (
                    kept[s, 1, :, columns].astype(f32) + sibling_recv[s, 1, :, columns].astype(f32)
                ).astype(bf16)
                peered[k, h] = send(
                    kept.at[s, 1, :, columns],
                    peer_recv.at[k - near, :, columns],
                    add_send.at[1 + h, k],
                    add_recv.at[1 + h, k],
                    rank,
                    peer,
                )
            return
        both = (kept[s].astype(f32) + sibling_recv[s].astype(f32)).astype(bf16)
        if k == 0:
            near_back[0] = both
            return
        kept[s] = both

    def give_back(k):
        backs[k] = send(
            kept.at[spot_of[k]],
            near_back.at[k],
            back_send.at[0, k],
            back_recv.at[0, k],
            partner(k),
            part,
        )

    def finish(k, h):
        s = spot_of[k]
        columns = halves[h]
        arrive(peered[k, h])
        kept[s, 0, :, columns] = (
            kept[s, 0, :, columns].astype(f32)
            + sibling_recv[s, 0, :, columns].astype(f32)
            + peer_recv[k - near, :, columns].astype(f32)
        ).astype(bf16)
        backs[k, h] = send(
            kept.at[s, 0, :, columns],
            far_back.at[k - near, :, columns],
            back_send.at[h, k],
            back_recv.at[h, k],
            partner(k),
            part,
        )

    def picked(j, source, first):
        count = source.shape[0]
        slots = lax.broadcasted_iota(i32, (quarter, count), 1) + first
        result = 0
        for i in range(TOP_K):
            hot = (spots[j, :, i : i + 1] == slots).astype(bf16)
            result = result + jnp.dot(hot, source, preferred_element_type=f32) * picks[
                j, :, i : i + 1
            ]
        return result

    def near_sum(j):
        if j:
            for k in range(1, near):
                arrive(backs[k])
            arrive(early["shared"])

        def one(c, carry):
            at = pl.ds(pl.multiple_of(c * chunk, chunk), chunk)
            source = near_back[:, j, :, at].reshape(near * share, chunk)
            value = (
                shared_part[j, :, at].astype(f32)
                + shared_recv[j, :, at].astype(f32)
                + picked(j, source, 0)
            )
            if j:
                merged_send[:, at] = value.astype(bf16)
            else:
                total[:, at] = value
            return carry

        lax.fori_loop(0, chunks, one, 0)
        if j:
            early["merged"] = send(
                merged_send, merged_recv, early_send.at[3], early_recv.at[3], rank, peer
            )

    def far_sum(first, count):
        last = first + count == ranks
        for k in range(first, first + count):
            for h in range(2):
                arrive(backs[k, h])
        if last:
            arrive(early["merged"])

        def one(c, carry):
            at = pl.ds(pl.multiple_of(c * chunk, chunk), chunk)
            source = far_back[first - near : first - near + count, :, at].reshape(
                count * share, chunk
            )
            value = total[:, at] + picked(0, source, first * share)
            if last:
                value = value + merged_recv[:, at].astype(f32)
                results[1, :, at] = value.astype(bf16)
            else:
                total[:, at] = value
            return carry

        if last:
            for c in range(chunks):
                one(c, 0)
                at = pl.ds(c * chunk, chunk)
                flushes.append(
                    load(results.at[1, :, at], outputs.at[1, :, at], flush_sem.at[c])
                )
        else:
            lax.fori_loop(0, chunks, one, 0)

    steps = {
        "proxy": proxy,
        "layouts": layouts,
        "norm": norm_tokens,
        "keys": keys,
        "attend": attend_half,
        "mixer": mixer,
        "shared": shared,
        "mixer_add": mixer_add,
        "mixer_finish": mixer_finish,
        "fan": fan,
        "relay": relay,
        "experts": experts,
        "add": add_pair,
        "back": give_back,
        "finish": finish,
        "near_sum": near_sum,
        "far_sum": far_sum,
    }
    for name, *settings in program:
        with jax.named_scope("_".join(map(str, (name, *settings)))):
            steps[name](*settings)
    for copy in sent:
        copy.wait_send()
    for copy in flushes:
        copy.wait()


def step_order(direct):
    program = (
        ("keys",), ("attend", 1), ("attend", 0), ("mixer", 1), ("mixer", 0), ("mixer_add",),
        ("proxy", 0), ("proxy", 1), ("fan", 3), ("fan", 0), ("relay", 4), ("experts", 4),
        ("fan", 5), ("fan", 2), ("relay", 3), ("experts", 2, 3), ("fan", 1), ("relay", 5),
        ("add", 4), ("fan", 6), ("add", 3), ("back", 3), ("experts", 5), ("finish", 4, 0),
        ("finish", 4, 1), ("add", 5), ("experts", 0, 1), ("add", 1), ("layouts",),
        ("mixer_finish",), ("norm", 3), ("relay", 6), ("finish", 5, 0), ("finish", 5, 1),
        ("fan", 7), ("experts", 6), ("back", 1), ("add", 2), ("back", 2), ("add", 6),
        ("relay", 7), ("norm", 2), ("finish", 6, 0), ("finish", 6, 1), ("experts", 7),
        ("shared",), ("add", 7), ("add", 0), ("near_sum", 1), ("finish", 7, 0),
        ("finish", 7, 1), ("near_sum", 0), ("far_sum", 4, 2), ("far_sum", 6, 1),
        ("far_sum", 7, 1),
    )
    return [step for step in program if step[0] != "relay" or step[1] >= direct]


def layer(arrays, local_experts, capacity, ranks):
    query_rows, out_weight, tokens, gate, up, down, shared_gate, shared_up, shared_down = arrays[1]
    near, direct = 4, 3
    order = tuple(range(ranks))
    bf16, f32 = jnp.bfloat16, jnp.float32
    dma = pltpu.SemaphoreType.DMA
    quarter = tokens.shape[0] // 4
    width = tokens.shape[1]
    share = local_experts * capacity
    sequence = query_rows.shape[0]
    far = ranks - near
    anywhere = pl.BlockSpec(memory_space=pl.ANY)
    smem = pl.BlockSpec(memory_space=pltpu.SMEM)

    def held(*shape):
        return pltpu.VMEM(shape, bf16)

    return pl.pallas_call(
        functools.partial(
            layer_kernel, ranks, near, direct, order, step_order(direct), local_experts, capacity
        ),
        out_shape=jax.ShapeDtypeStruct((2, quarter, width), bf16),
        in_specs=[smem]
        + [anywhere] * 3
        + [anywhere] * 13,
        out_specs=anywhere,
        scratch_shapes=[
            held(2, quarter, width),
            dma((width // 512 + 1,)),
            pltpu.VMEM((1, HEAD_DIM), f32),
            pltpu.VMEM((1, HEAD_DIM), f32),
            dma((2,)),
            held(ranks, 4, share, width),
            held(ranks, 2, share, width),
            held(ranks, 2, share, width),
            held(ranks, 2, share, width),
            held(far, share, width),
            held(far - 1, share, width),
            held(near - 1, 2, share, width),
            held(far, share, width),
            held(near, 2, share, width),
            held(4, quarter, width),
            held(4, quarter, width),
            held(2, quarter, width),
            held(2, quarter, width),
            held(quarter, width),
            held(quarter, width),
            held(quarter, width),
            held(quarter, width),
            pltpu.VMEM((quarter, width), f32),
            held(4, quarter, width),
            held(*query_rows.shape),
            held(sequence + BLOCK, 128),
            held(sequence + BLOCK, 128),
            held(2, 2, sequence + BLOCK, 128),
            held(2, 2, sequence + BLOCK, 128),
            held(4, quarter, query_rows.shape[1]),
            pltpu.VMEM((2, TOP_K, quarter), jnp.int32),
            pltpu.VMEM((2, TOP_K, quarter), f32),
            pltpu.VMEM((2, quarter, TOP_K), jnp.int32),
            pltpu.VMEM((2, quarter, TOP_K), f32),
            pltpu.VMEM((1, width), f32),
            held(quarter, width),
            pltpu.VMEM((TOP_K, quarter), jnp.int32),
            held(*gate.shape),
            held(*up.shape),
            held(*down.shape),
            held(*out_weight.shape),
            held(*shared_gate.shape),
            held(*shared_up.shape),
            held(*shared_down.shape),
            dma((4,)),
            dma((8,)),
            dma((7,)),
            dma((3,)),
            dma((3,)),
            dma((2, ranks)),
            dma((2, ranks)),
            dma((5, ranks)),
            dma((5, ranks)),
            dma((3, ranks)),
            dma((3, ranks)),
            dma((2, ranks)),
            dma((2, ranks)),
            dma((5,)),
            dma((5,)),
        ],
        compiler_params=pltpu.CompilerParams(
            collective_id=0, has_side_effects=True, vmem_limit_bytes=65000 * 1024
        ),
    )(*arrays[0])


def wide_shards(
    query_rows,
    key_rows,
    value_rows,
    query_gain,
    key_gain,
    sink_logit,
    out_weight,
    tokens,
    norm_gain,
    expert_ids,
    route_weight,
    gate_weight,
    up_weight,
    down_weight,
    shared_gate,
    shared_up,
    shared_down,
):
    expert_ranks = lax.axis_size("ep")
    head_ranks = lax.axis_size("tp")
    head_rank = lax.axis_index("tp")
    sequence_rows = query_rows.shape[0]
    blocks = sequence_rows // BLOCK
    pair_heads = key_rows.shape[1] // HEAD_DIM
    group_size = HEADS // KV_HEADS
    query_normed = rms_scale(
        query_rows.reshape(blocks, BLOCK, pair_heads, group_size, HEAD_DIM), query_gain
    )
    key_normed = rms_scale(key_rows.reshape(blocks, BLOCK, pair_heads, HEAD_DIM), key_gain)
    value_blocks = value_rows.reshape(blocks, BLOCK, pair_heads, HEAD_DIM)
    rim_keys, rim_values = from_behind((key_normed[blocks - 1], value_blocks[blocks - 1]), "ep", 1)
    key_band = band_blocks(rim_keys, key_normed)
    value_band = band_blocks(rim_values, value_blocks)
    window = window_mask(lax.axis_index("ep") * blocks, blocks)
    scores = (
        jnp.einsum("nqhgd,nkhd->hgnqk", query_normed, key_band, preferred_element_type=jnp.float32)
        * score_scale
    )
    scores = jnp.where(window[None, None], scores, masked_score)
    sink_col = sink_logit.reshape(pair_heads, group_size, 1, 1, 1)
    row_max = jnp.maximum(jnp.max(scores, axis=-1, keepdims=True), sink_col)
    exp_scores = jnp.exp(scores - row_max)
    attn_probs = (
        exp_scores / (jnp.sum(exp_scores, axis=-1, keepdims=True) + jnp.exp(sink_col - row_max))
    ).astype(jnp.bfloat16)
    heads_out = (
        jnp.einsum("hgnqk,nkhd->nqhgd", attn_probs, value_band, preferred_element_type=jnp.float32)
        .astype(jnp.bfloat16)
        .reshape(sequence_rows, pair_heads * group_size * HEAD_DIM)
    )
    local_experts = gate_weight.shape[0]
    expert_total = local_experts * expert_ranks
    quarter = tokens.shape[0] // head_ranks
    model_width = tokens.shape[1]
    capacity = 2 * quarter * TOP_K // expert_total
    slot_share = local_experts * capacity
    routed_rows = expert_ranks * slot_share
    normed = rms_scale(tokens, norm_gain)
    route_ids = expert_ids.reshape(head_ranks, quarter * TOP_K)
    one_hot = (route_ids[:, :, None] == jnp.arange(expert_total, dtype=jnp.int32)).astype(jnp.int32)
    slot_rank = jnp.sum(one_hot * (jnp.cumsum(one_hot, axis=1) - 1), axis=-1)
    positions = route_ids * capacity + slot_rank
    owners = jnp.arange(quarter * TOP_K, dtype=jnp.int32) // TOP_K
    padded_rows = jnp.concatenate(
        [
            normed.reshape(head_ranks, quarter, model_width),
            jnp.zeros((head_ranks, 1, model_width), jnp.bfloat16),
        ],
        axis=1,
    ).reshape(head_ranks * (quarter + 1), model_width)
    slot_token = (
        jnp.full((head_ranks, routed_rows), quarter, jnp.int32)
        .at[jnp.arange(head_ranks, dtype=jnp.int32)[:, None], positions]
        .set(jnp.broadcast_to(owners[None, :], positions.shape))
    )
    slot_index = slot_token + (jnp.arange(head_ranks, dtype=jnp.int32) * (quarter + 1))[:, None]
    own_index = lax.dynamic_index_in_dim(slot_index, head_rank, 0, keepdims=True)
    outgoing = padded_rows[own_index].reshape(1, expert_ranks, slot_share, model_width)
    arrived = lax.all_to_all(outgoing, "ep", split_axis=1, concat_axis=1, tiled=True)
    piece_rows = lax.all_gather(
        arrived.reshape(1, expert_ranks, local_experts, capacity, model_width),
        "tp",
        axis=0,
        tiled=True,
    )
    gate_part = jnp.einsum(
        "tsecd,edf->tsecf", piece_rows, gate_weight, preferred_element_type=jnp.float32
    )
    up_part = jnp.einsum(
        "tsecd,edf->tsecf", piece_rows, up_weight, preferred_element_type=jnp.float32
    )
    hidden = (jax.nn.silu(gate_part) * up_part).astype(jnp.bfloat16)
    shared_hidden = (
        jax.nn.silu(jnp.dot(normed, shared_gate, preferred_element_type=jnp.float32))
        * jnp.dot(normed, shared_up, preferred_element_type=jnp.float32)
    ).astype(jnp.bfloat16)
    span_rows = routed_rows + quarter
    mixer_out = lax.psum_scatter(
        jnp.dot(heads_out, out_weight, preferred_element_type=jnp.float32).astype(jnp.bfloat16),
        "tp",
        scatter_dimension=0,
        tiled=True,
    )
    part_count = lax.axis_size("tp") * span_rows // span_rows
    routed_part = jnp.einsum(
        "tsecf,efd->tsecd", hidden, down_weight, preferred_element_type=jnp.float32
    ).reshape(part_count, routed_rows, model_width)
    shared_part = jnp.dot(shared_hidden, shared_down, preferred_element_type=jnp.float32).reshape(
        part_count, quarter, model_width
    )
    summed = lax.psum_scatter(
        jnp.concatenate([routed_part, shared_part], axis=1)
        .reshape(part_count * span_rows, model_width)
        .astype(jnp.bfloat16),
        "tp",
        scatter_dimension=0,
        tiled=True,
    )
    returned = lax.all_to_all(
        summed[:routed_rows].reshape(expert_ranks, slot_share, model_width),
        "ep",
        split_axis=0,
        concat_axis=0,
        tiled=True,
    ).reshape(routed_rows, model_width)
    own_positions = lax.dynamic_index_in_dim(positions, head_rank, 0, keepdims=False)
    picked = returned[own_positions].reshape(quarter, TOP_K, model_width).astype(jnp.float32)
    own_weights = lax.dynamic_slice_in_dim(route_weight, head_rank * quarter, quarter, 0)
    expert_out = (
        summed[routed_rows:].astype(jnp.float32) + jnp.sum(picked * own_weights[:, :, None], axis=1)
    ).astype(jnp.bfloat16)
    return (mixer_out, expert_out)


def shards(
    query_rows,
    key_rows,
    value_rows,
    query_gain,
    key_gain,
    sink_logit,
    out_weight,
    tokens,
    norm_gain,
    expert_ids,
    route_weight,
    gate_weight,
    up_weight,
    down_weight,
    shared_gate,
    shared_up,
    shared_down,
):
    expert_ranks = lax.axis_size("ep")
    head_ranks = lax.axis_size("tp")
    local_experts = gate_weight.shape[0]
    expert_total = local_experts * expert_ranks
    quarter = tokens.shape[0] // head_ranks
    capacity = 2 * quarter * TOP_K // expert_total
    fits = (
        head_ranks == 4
        and expert_ranks == 8
        and capacity % 16 == 0
        and quarter == BLOCK
        and query_rows.shape[0] == 4 * BLOCK
        and key_rows.shape[1] == 2 * HEAD_DIM
    )
    if not fits:
        return wide_shards(
            query_rows,
            key_rows,
            value_rows,
            query_gain,
            key_gain,
            sink_logit,
            out_weight,
            tokens,
            norm_gain,
            expert_ids,
            route_weight,
            gate_weight,
            up_weight,
            down_weight,
            shared_gate,
            shared_up,
            shared_down,
        )
    operands = (
        sink_logit,
        query_rows,
        key_rows,
        value_rows,
        query_gain.reshape(1, HEAD_DIM),
        key_gain.reshape(1, HEAD_DIM),
        out_weight,
        tokens,
        norm_gain.reshape(1, tokens.shape[1]),
        expert_ids.T,
        route_weight.T,
        gate_weight,
        up_weight,
        down_weight,
        shared_gate,
        shared_up,
        shared_down,
    )
    shaped = (
        query_rows,
        out_weight,
        tokens,
        gate_weight,
        up_weight,
        down_weight,
        shared_gate,
        shared_up,
        shared_down,
    )
    both = layer((operands, shaped), local_experts, capacity, expert_ranks)
    return both[0], both[1]


def solution(mesh):
    in_specs = (
        P("ep", "tp"),
        P("ep", "tp"),
        P("ep", "tp"),
        P(),
        P(),
        P("tp"),
        P("tp", None),
        P("ep", None),
        P(),
        P("ep", None),
        P("ep", None),
        P("ep", None, "tp"),
        P("ep", None, "tp"),
        P("ep", "tp", None),
        P(None, "tp"),
        P(None, "tp"),
        P("tp", None),
    )
    out_specs = (P(("ep", "tp"), None), P(("ep", "tp"), None))
    return jax.shard_map(shards, mesh=mesh, in_specs=in_specs, out_specs=out_specs, check_vma=False)
```
